128 devices in a mesh: rep: 2 (over z_hi), fs: 32 (over z_lo, y, x), tp: 2 (over core).
Axes of the slice: x: 4, y: 4, z: 4 (z_hi: 2, z_lo: 2; z = z_hi * 2 + z_lo), core: 2. Of those that a mesh axis runs over, the one named last changes fastest.
Arguments:
- tokens: bfloat16 [65536, 2048], P(('rep', 'fs', 'tp')), parts along dimension 0, may hold values from -6 to 6
- mix_gain: float32 [2048], replicated, may hold values from 0.1 to 1.9
- w_query: bfloat16 [2048, 512], P('fs', 'tp'), may hold values from -0.125 to 0.125
- w_key: bfloat16 [2048, 512], P('fs', 'tp'), may hold values from -0.125 to 0.125
- w_value: bfloat16 [2048, 1024], P('fs', 'tp'), may hold values from -0.125 to 0.125
- w_out: bfloat16 [1024, 2048], P('tp', 'fs'), may hold values from -0.1875 to 0.1875
- ffn_gain: float32 [2048], replicated, may hold values from 0.1 to 1.9
- w_ffgate: bfloat16 [2048, 2816], P('fs', 'tp'), may hold values from -0.125 to 0.125
- w_ffup: bfloat16 [2048, 2816], P('fs', 'tp'), may hold values from -0.125 to 0.125
- conv_gate: float32 [3, 2816], replicated, may hold values from -3 to 3
- conv_up: float32 [3, 2816], replicated, may hold values from -3 to 3
- w_down: bfloat16 [2816, 2048], P('tp', 'fs'), may hold values from -0.109375 to 0.109375
Outputs:
- layer_out: bfloat16 [65536, 2048], P(('rep', 'fs', 'tp')), parts along dimension 0
The draws below stay inside these ranges and needn't reach their ends.
There are 2 independent parts, one for each index of `rep`. The reference program is written for one: setup_inputs(seed, part) draws one part's arguments, and reference() takes and returns one part's arrays. A program takes and returns all parts, laid end to end along the dimension named above; an argument that names none is the same for every part. Nothing has to cross between parts.
All inputs are finite; a program needn't handle non-finite values.
Results may differ from the reference program's by a relative error of at most 0.014.
Values may be sent and summed in bfloat16 or wider, within the bound.
A program may use at most 128 MiB of HBM per device.

```python
import jax
import jax.numpy as jnp
from jax import lax

D = 2048
HEADS = 4
DK = 128
DV = 256
FF = 2816
KERNEL = 3
BLOCK = 128
LENGTH = 1024
TOKENS = 32768
N_TP = 2


def levels(key, shape, split, low, largest):
    level, own = 1.0, jax.random.fold_in(key, 6)
    for position, shards_of in split:
        draws = jnp.exp(jax.random.uniform(jax.random.fold_in(own, position), (shards_of,), jnp.float32, low / len(split), largest / len(split)))
        level = level * jnp.repeat(draws, shape[position] // shards_of).reshape([-1 if axis == position else 1 for axis in range(len(shape))])
    return level


def bell_draw(key, dims, scale, most, shards=(), kind=jnp.bfloat16):
    level = levels(key, dims, shards, -0.22, 0.18) if shards else 1.0
    drawn = jax.random.normal(key, dims, jnp.float32) * scale * level
    return jnp.minimum(jnp.maximum(drawn, -most), most).astype(kind)


def setup_inputs(seed: int = 0, part: int = 0) -> dict:
    arg_keys = jax.random.split(jax.random.key(seed), 13)
    part_keys = jax.random.split(jax.random.fold_in(arg_keys[12], part), 13)
    return {
        "tokens": bell_draw(part_keys[0], (TOKENS, D), 1.0, 6.0, ((0, 64),)),
        "mix_gain": jnp.clip(1.0 + 0.18 * jax.random.normal(arg_keys[1], (D,), jnp.float32), 0.1, 1.9),
        "w_query": bell_draw(arg_keys[2], (D, HEADS * DK), D ** -0.5, 0.125, ((0, 32), (1, 2))),
        "w_key": bell_draw(arg_keys[3], (D, HEADS * DK), D ** -0.5, 0.125, ((0, 32), (1, 2))),
        "w_value": bell_draw(arg_keys[4], (D, HEADS * DV), D ** -0.5, 0.125, ((0, 32), (1, 2))),
        "w_out": bell_draw(arg_keys[5], (HEADS * DV, D), (HEADS * DV) ** -0.5, 0.1875, ((0, 2), (1, 32))),
        "ffn_gain": jnp.clip(1.0 + 0.18 * jax.random.normal(arg_keys[6], (D,), jnp.float32), 0.1, 1.9),
        "w_ffgate": bell_draw(arg_keys[7], (D, FF), D ** -0.5, 0.125, ((0, 32), (1, 2))),
        "w_ffup": bell_draw(arg_keys[8], (D, FF), D ** -0.5, 0.125, ((0, 32), (1, 2))),
        "conv_gate": bell_draw(arg_keys[9], (KERNEL, FF), 0.58, 3.0, (), jnp.float32),
        "conv_up": bell_draw(arg_keys[10], (KERNEL, FF), 0.58, 3.0, (), jnp.float32),
        "w_down": bell_draw(arg_keys[11], (FF, D), FF ** -0.5, 0.109375, ((0, 2), (1, 32))),
    }


epsilon = 1e-06

def rms_rows(matrix, scale_vec):
    values = matrix.astype(jnp.float32)
    factor = lax.rsqrt(lax.optimization_barrier(jnp.mean(values * values, axis=-1, keepdims=True)) + epsilon)
    return (values * factor * scale_vec).astype(jnp.bfloat16)

def rotate_heads(matrix):
    length = matrix.shape[0]
    half_width = matrix.shape[-1] // 2
    inverse = 10000.0 ** (-jnp.arange(half_width, dtype=jnp.float32) * 2.0 / (2 * half_width))
    angles = jnp.arange(length, dtype=jnp.float32)[:, None] * inverse[None, :]
    cosine = jnp.cos(angles)[:, None, :]
    sine = jnp.sin(angles)[:, None, :]
    values = matrix.astype(jnp.float32)
    first_half = values[..., :half_width]
    second_half = values[..., half_width:]
    return jnp.concatenate([first_half * cosine - second_half * sine, first_half * sine + second_half * cosine], axis=-1)

def retain_blocks(rot_query, rot_key, value, rates, block_len):
    length, head_count, width_k = rot_query.shape
    width_v = value.shape[-1]
    blocks = length // block_len
    query4 = rot_query.reshape(blocks, block_len, head_count, width_k).astype(jnp.float32)
    key4 = rot_key.reshape(blocks, block_len, head_count, width_k)
    value4 = value.reshape(blocks, block_len, head_count, width_v).astype(jnp.float32)
    places = jnp.arange(block_len, dtype=jnp.float32)
    spacing = places[:, None] - places[None, :]
    inside = jnp.where(spacing[None] >= 0, jnp.exp(-jnp.maximum(spacing, 0.0)[None] * rates[:, None, None]), 0.0)
    scores = jnp.einsum('cihd,cjhd->chij', query4, key4.astype(jnp.float32), precision=lax.Precision.HIGHEST)
    weights = (scores * inside[None]).astype(jnp.bfloat16)
    inner_part = jnp.einsum('chij,cjhe->cihe', weights.astype(jnp.float32), value4, precision=lax.Precision.HIGHEST)
    tail_decay = jnp.exp(-(block_len - 1.0 - places)[:, None] * rates[None, :])
    decayed = (key4.astype(jnp.float32) * tail_decay[None, :, :, None]).astype(jnp.bfloat16)
    states = jnp.einsum('cjhd,cjhe->chde', decayed.astype(jnp.float32), value4, precision=lax.Precision.HIGHEST)
    passing = jnp.exp(-block_len * rates)[:, None, None]

    def advance(carried, fresh):
        return (carried * passing + fresh, carried)
    _, before = lax.scan(advance, jnp.zeros((head_count, width_k, width_v), jnp.float32), states)
    onset_decay = jnp.exp(-(places + 1.0)[:, None] * rates[None, :])
    cross_part = jnp.einsum('cihd,chde->cihe', query4, before, precision=lax.Precision.HIGHEST) * onset_decay[None, :, :, None]
    return (inner_part + cross_part).reshape(length, head_count, width_v)

def head_norm(retained):
    average = lax.optimization_barrier(jnp.mean(retained, axis=-1, keepdims=True))
    centered = retained - average
    return centered * lax.rsqrt(lax.optimization_barrier(jnp.mean(centered * centered, axis=-1, keepdims=True)) + epsilon)

def group_sum(hidden, weight):
    width = hidden.shape[1] // N_TP
    total = jnp.zeros((hidden.shape[0], weight.shape[1]), jnp.float32)
    for section in range(N_TP):
        partial_sum = jnp.dot(hidden[:, section * width:(section + 1) * width], weight[section * width:(section + 1) * width], preferred_element_type=jnp.float32).astype(jnp.bfloat16)
        partial_sum = lax.optimization_barrier(partial_sum)
        total = total + partial_sum.astype(jnp.float32)
    return total

def causal_taps(matrix, kernel_w):
    length = matrix.shape[0]
    padded = jnp.pad(matrix.astype(jnp.float32), ((KERNEL - 1, 0), (0, 0)))
    total = jnp.zeros((length, matrix.shape[1]), jnp.float32)
    for tap_idx in range(KERNEL):
        total = total + kernel_w[tap_idx][None, :] * padded[tap_idx:tap_idx + length]
    return total

def reference(tokens, mix_gain, w_query, w_key, w_value, w_out, ffn_gain, w_ffgate, w_ffup, conv_gate, conv_up, w_down):
    sequences = tokens.reshape(TOKENS // LENGTH, LENGTH, D)

    def layer(rows):
        normed = rms_rows(rows, mix_gain)
        query = jnp.dot(normed, w_query, preferred_element_type=jnp.float32).astype(jnp.bfloat16)
        key = jnp.dot(normed, w_key, preferred_element_type=jnp.float32).astype(jnp.bfloat16)
        value = jnp.dot(normed, w_value, preferred_element_type=jnp.float32).astype(jnp.bfloat16)
        rot_query = rotate_heads(query.reshape(LENGTH, HEADS, DK)).astype(jnp.bfloat16)
        rot_key = (rotate_heads(key.reshape(LENGTH, HEADS, DK)) * DK ** (-0.5)).astype(jnp.bfloat16)
        rates = 1.0 / 16.0 * (32.0 / LENGTH) ** (jnp.arange(HEADS, dtype=jnp.float32) / (HEADS - 1))
        retained = retain_blocks(rot_query, rot_key, value.reshape(LENGTH, HEADS, DV), rates, BLOCK)
        hidden = head_norm(retained).reshape(LENGTH, HEADS * DV).astype(jnp.bfloat16)
        mix_sum = group_sum(hidden, w_out)
        resid = (rows.astype(jnp.float32) + mix_sum).astype(jnp.bfloat16)
        normed_ffn = rms_rows(resid, ffn_gain)
        gate_pre = jnp.dot(normed_ffn, w_ffgate, preferred_element_type=jnp.float32).astype(jnp.bfloat16)
        up_pre = jnp.dot(normed_ffn, w_ffup, preferred_element_type=jnp.float32).astype(jnp.bfloat16)
        activ = (jax.nn.silu(causal_taps(gate_pre, conv_gate)) * causal_taps(up_pre, conv_up)).astype(jnp.bfloat16)
        ffn_sum = group_sum(activ, w_down)
        return (resid.astype(jnp.float32) + ffn_sum).astype(jnp.bfloat16)
    return lax.map(layer, sequences).reshape(TOKENS, D)
```

```python
import jax
import jax.numpy as jnp
from jax import lax
from jax.experimental import pallas as pl
from jax.experimental.pallas import tpu as pltpu
from jax.sharding import PartitionSpec as P

MESH = pl.DeviceIdType.MESH
C = 23
COLS = 256
LAG = 2

HEADS = 4
DK = 128
DV = 256
KERNEL = 3
BLOCK = 128
LENGTH = 1024


epsilon = 1e-06


def place():
    rep = lax.axis_index("rep"); fs = lax.axis_index("fs"); tp = lax.axis_index("tp")
    zl = fs // 16; y = (fs // 4) % 4; x = fs % 4
    z = rep * 2 + zl
    def dev(z_, y_, x_):
        return (z_ // 2, (z_ % 2) * 16 + y_ * 4 + x_, tp)
    xp, xm, yp, ym = (x + 1) % 4, (x + 3) % 4, (y + 1) % 4, (y + 3) % 4
    zp, zm = (z + 1) % 4, (z + 3) % 4
    to = dict(xp=dev(z, y, xp), xm=dev(z, y, xm), yp=dev(z, yp, x), ym=dev(z, ym, x), zp=dev(zp, y, x), zm=dev(zm, y, x))
    partner = (rep, fs, 1 - tp)
    return zl, y, x, xp, xm, yp, ym, to, partner

def make_comm(W, send_sem, recv_sem):
    zl, y, x, xp, xm, yp, ym, to, partner = place()
    A = pl.ds(0, 16); B = pl.ds(16, 16); Cc = pl.ds(32, 16); D = pl.ds(48, 16)
    lo, hi = pl.ds(0, 2), pl.ds(2, 2)
    al = slice(None)
    def put(c, stage, sg, idx, d):
        r = W.at[(c,) + idx]
        pltpu.make_async_remote_copy(src_ref=r, dst_ref=r, send_sem=send_sem.at[sg], recv_sem=recv_sem.at[c, stage],
            device_id=to[d], device_id_type=MESH).start()
    def send(c, s):
        if s == 0:
            for d in ("xp", "xm"): put(c, 0, 0, (zl, y, x, pl.ds(0, 32)), d)
            for d in ("yp", "ym"): put(c, 0, 0, (zl, y, x, pl.ds(32, 32)), d)
        elif s == 1:
            put(c, 1, 1, (zl, y, xm, A), "xp")
            put(c, 1, 1, (zl, y, xp, B), "xm")
            put(c, 1, 1, (zl, ym, x, Cc), "yp")
            put(c, 1, 1, (zl, yp, x, D), "ym")
        elif s == 2:
            for d in ("yp", "ym"): put(c, 2, 2, (zl, y, al, A), d)
            for d in ("xp", "xm"): put(c, 2, 2, (zl, al, x, Cc), d)
            put(c, 2, 2, (zl, y, lo, B), "zp")
            put(c, 2, 2, (zl, y, hi, B), "zm")
            put(c, 2, 2, (zl, lo, x, D), "zp")
            put(c, 2, 2, (zl, hi, x, D), "zm")
        elif s == 3:
            for d in ("yp", "ym"): put(c, 3, 4, (al, y, al, B), d)
            for d in ("xp", "xm"): put(c, 3, 4, (al, al, x, D), d)
            put(c, 3, 3, (zl, ym, lo, A), "yp")
            put(c, 3, 3, (zl, yp, hi, A), "ym")
            put(c, 3, 3, (zl, lo, xm, Cc), "xp")
            put(c, 3, 3, (zl, hi, xp, Cc), "xm")
        elif s == 4:
            put(c, 4, 5, (zl, lo, al, A), "zp")
            put(c, 4, 5, (zl, hi, al, A), "zm")
            put(c, 4, 5, (zl, al, lo, Cc), "zp")
            put(c, 4, 5, (zl, al, hi, Cc), "zm")
            put(c, 4, 5, (0, ym, al, B), "yp")
            put(c, 4, 5, (1, yp, al, B), "ym")
            put(c, 4, 5, (0, al, xm, D), "xp")
            put(c, 4, 5, (1, al, xp, D), "xm")
    def waitn(ref, sem):
        pltpu.make_async_copy(ref, ref, sem).wait()
    def arrived(c, s):
        r = [W.at[c, 0, 0, pl.ds(0, 2)], W.at[c, 0, 0, 0], W.at[c, 0, pl.ds(0, 3), pl.ds(0, 2)],
             W.at[pl.ds(0, 5), 0, 0, pl.ds(0, 2)], W.at[c, 0, pl.ds(0, 3)]][s]
        waitn(r, recv_sem.at[c, s])
    def drain():
        for i, r in enumerate([W.at[:, 0, 0, pl.ds(0, 2)], W.at[:, 0, 0, 0], W.at[:, 0, pl.ds(0, 3), pl.ds(0, 2)],
                 W.at[:, 0, 0, pl.ds(0, 2)], W.at[:, :, 0], W.at[:, 0, pl.ds(0, 3)]]):
            waitn(r, send_sem.at[i])
    def tick(t):
        for s in range(6):
            c = t - LAG * s
            @pl.when((c >= 0) & (c < C))
            def _():
                if s:
                    arrived(c, s - 1)
                if s < 5:
                    send(c, s)
    return tick, drain, (zl, y, x, to, partner)

def barrier(to, partner):
    b = pltpu.get_barrier_semaphore()
    for d in list(to.values()) + [partner]:
        pl.semaphore_signal(b, inc=1, device_id=d, device_id_type=MESH)
    pl.semaphore_wait(b, 7)


def kernel(src, W, send_sem, recv_sem, lsem):
    tick, drain, (zl, y, x, to, partner) = make_comm(W, send_sem, recv_sem)
    own = pltpu.make_async_copy(src, W.at[:, zl, y, x], lsem)
    own.start()
    barrier(to, partner)
    own.wait()
    lax.fori_loop(0, C + 5 * LAG, lambda t, _: (tick(t), 0)[1], 0)
    drain()


def gather(src):
    return pl.pallas_call(
        kernel,
        out_shape=jax.ShapeDtypeStruct((C, 2, 4, 4, 64, COLS), jnp.bfloat16),
        in_specs=[pl.BlockSpec(memory_space=pltpu.VMEM)],
        out_specs=pl.BlockSpec(memory_space=pl.ANY),
        scratch_shapes=[
            pltpu.SemaphoreType.DMA((6,)),
            pltpu.SemaphoreType.DMA((C, 5)),
            pltpu.SemaphoreType.DMA,
        ],
        compiler_params=pltpu.CompilerParams(collective_id=0, has_side_effects=True),
    )(src)


def own_chunks(w_query, w_key, w_value, w_out, w_ffgate, w_ffup, w_down):
    parts = []
    for h in range(2):
        parts += [w_query[:, h * 128 : h * 128 + 128], w_key[:, h * 128 : h * 128 + 128], w_value[:, h * 256 : h * 256 + 256]]
    parts.append(w_out.T)
    for j in range(11):
        parts += [w_ffgate[:, j * 128 : j * 128 + 128], w_ffup[:, j * 128 : j * 128 + 128]]
    parts += [w_down.T, jnp.zeros((64, 128), jnp.bfloat16)]
    flat = jnp.concatenate(parts, axis=1)
    return jnp.transpose(flat.reshape(64, C, COLS), (1, 0, 2))


def in_blocks(shard, dim, length):
    dims = shard.shape
    pieces = shard.reshape(*dims[:dim], length, dims[dim] // length, *dims[dim + 1 :])
    return jnp.moveaxis(pieces, dim, 0)


def sent_and_summed(shard, axis, dim):
    length = lax.axis_size(axis)
    pieces = lax.all_to_all(in_blocks(shard, dim, length), axis, 0, 0, tiled=True)
    return jnp.sum(pieces.astype(jnp.float32), axis=0)


def rms_rows(matrix, scale_vec):
    values = matrix.astype(jnp.float32)
    factor = lax.rsqrt(jnp.mean(values * values, axis=-1, keepdims=True) + epsilon)
    return (values * factor * scale_vec).astype(jnp.bfloat16)


def rotate_heads(matrix):
    length = matrix.shape[0]
    half_width = matrix.shape[-1] // 2
    inverse = 10000.0 ** (-jnp.arange(half_width, dtype=jnp.float32) * 2.0 / (2 * half_width))
    angles = jnp.arange(length, dtype=jnp.float32)[:, None] * inverse[None, :]
    cosine = jnp.cos(angles)[:, None, :]
    sine = jnp.sin(angles)[:, None, :]
    values = matrix.astype(jnp.float32)
    first_half = values[..., :half_width]
    second_half = values[..., half_width:]
    return jnp.concatenate(
        [first_half * cosine - second_half * sine, first_half * sine + second_half * cosine],
        axis=-1,
    )


def retain_blocks(rot_query, rot_key, value, rates, block_len):
    length, head_count, width_k = rot_query.shape
    width_v = value.shape[-1]
    blocks = length // block_len
    query4 = rot_query.reshape(blocks, block_len, head_count, width_k)
    key4 = rot_key.reshape(blocks, block_len, head_count, width_k)
    value4 = value.reshape(blocks, block_len, head_count, width_v)
    places = jnp.arange(block_len, dtype=jnp.float32)
    spacing = places[:, None] - places[None, :]
    inside = jnp.where(
        spacing[None] >= 0, jnp.exp(-jnp.maximum(spacing, 0.0)[None] * rates[:, None, None]), 0.0
    )
    scores = jnp.einsum("cihd,cjhd->chij", query4, key4, preferred_element_type=jnp.float32)
    weights = (scores * inside[None]).astype(jnp.bfloat16)
    inner_part = jnp.einsum("chij,cjhe->cihe", weights, value4, preferred_element_type=jnp.float32)
    tail_decay = jnp.exp(-(block_len - 1.0 - places)[:, None] * rates[None, :])
    decayed = (key4.astype(jnp.float32) * tail_decay[None, :, :, None]).astype(jnp.bfloat16)
    states = jnp.einsum("cjhd,cjhe->chde", decayed, value4, preferred_element_type=jnp.float32)
    passing = jnp.exp(-block_len * rates)[:, None, None]

    def advance(carried, fresh):
        return (carried * passing + fresh, carried)

    _, before = lax.scan(advance, jnp.zeros((head_count, width_k, width_v), jnp.float32), states)
    onset_decay = jnp.exp(-(places + 1.0)[:, None] * rates[None, :])
    cross_part = (
        jnp.einsum("cihd,chde->cihe", query4.astype(jnp.float32), before)
        * onset_decay[None, :, :, None]
    )
    return (inner_part + cross_part).reshape(length, head_count, width_v)


def head_norm(retained):
    average = jnp.mean(retained, axis=-1, keepdims=True)
    centered = retained - average
    return centered * lax.rsqrt(jnp.mean(centered * centered, axis=-1, keepdims=True) + epsilon)


def causal_taps(matrix, kernel_w):
    length = matrix.shape[0]
    padded = jnp.pad(matrix.astype(jnp.float32), ((KERNEL - 1, 0), (0, 0)))
    total = jnp.zeros((length, matrix.shape[1]), jnp.float32)
    for tap_idx in range(KERNEL):
        total = total + kernel_w[tap_idx][None, :] * padded[tap_idx : tap_idx + length]
    return total


def body(
    tokens,
    mix_gain,
    w_query,
    w_key,
    w_value,
    w_out,
    ffn_gain,
    w_ffgate,
    w_ffup,
    conv_gate,
    conv_up,
    w_down,
):
    tp_rank = lax.axis_index("tp")
    heads_here = w_query.shape[1] // DK
    normed = rms_rows(tokens, mix_gain)
    full = gather(own_chunks(w_query, w_key, w_value, w_out, w_ffgate, w_ffup, w_down)).reshape(C, 2048, COLS)
    qk_cols = w_query.shape[1]
    pieces = lax.all_gather(normed, "tp", axis=0, tiled=True)
    heads = jnp.einsum("mk,ckn->cmn", pieces, full[:4], preferred_element_type=jnp.float32).astype(jnp.bfloat16)
    joined = jnp.concatenate(
        [heads[0, :, :128], heads[2, :, :128], heads[0, :, 128:], heads[2, :, 128:], heads[1], heads[3]], axis=1
    )
    length = joined.shape[0]
    query = joined[:, :qk_cols].reshape(length, heads_here, DK)
    key = joined[:, qk_cols : 2 * qk_cols].reshape(length, heads_here, DK)
    value = joined[:, 2 * qk_cols :].reshape(length, heads_here, DV)
    rot_query = rotate_heads(query).astype(jnp.bfloat16)
    rot_key = (rotate_heads(key) * DK ** (-0.5)).astype(jnp.bfloat16)
    head_ids = (tp_rank * heads_here + jnp.arange(heads_here, dtype=jnp.int32)).astype(jnp.float32)
    rates = 1.0 / 16.0 * (32.0 / LENGTH) ** (head_ids / (HEADS - 1))
    retained = retain_blocks(rot_query, rot_key, value, rates, BLOCK)
    hidden = head_norm(retained).reshape(length, heads_here * DV).astype(jnp.bfloat16)
    out_full = jnp.concatenate([full[4], full[5]], axis=1).T
    mix_sum = sent_and_summed(
        jnp.dot(hidden, out_full, preferred_element_type=jnp.float32).astype(jnp.bfloat16), "tp", 0
    )
    resid = (tokens.astype(jnp.float32) + mix_sum).astype(jnp.bfloat16)
    normed_ffn = rms_rows(resid, ffn_gain)
    ff_here = w_ffgate.shape[1]
    pieces = lax.all_gather(normed_ffn, "tp", axis=0, tiled=True)
    both = jnp.einsum("mk,ckn->mcn", pieces, full[6:17], preferred_element_type=jnp.float32).astype(jnp.bfloat16)
    gate_pre = both[:, :, :128].reshape(length, ff_here)
    up_pre = both[:, :, 128:].reshape(length, ff_here)
    gate_taps = lax.dynamic_slice_in_dim(conv_gate, tp_rank * ff_here, ff_here, 1)
    up_taps = lax.dynamic_slice_in_dim(conv_up, tp_rank * ff_here, ff_here, 1)
    activ = (jax.nn.silu(causal_taps(gate_pre, gate_taps)) * causal_taps(up_pre, up_taps)).astype(
        jnp.bfloat16
    )
    down_full = jnp.concatenate([full[i] for i in range(17, 23)], axis=1)[:, :ff_here].T
    ffn_sum = sent_and_summed(
        jnp.dot(activ, down_full, preferred_element_type=jnp.float32).astype(jnp.bfloat16), "tp", 0
    )
    return (resid.astype(jnp.float32) + ffn_sum).astype(jnp.bfloat16)


def solution(mesh):
    placed = (
        P(("rep", "fs", "tp"), None),
        P(),
        P("fs", "tp"),
        P("fs", "tp"),
        P("fs", "tp"),
        P("tp", "fs"),
        P(),
        P("fs", "tp"),
        P("fs", "tp"),
        P(),
        P(),
        P("tp", "fs"),
    )
    return jax.shard_map(
        body, mesh=mesh, in_specs=placed, out_specs=P(("rep", "fs", "tp"), None), check_vma=False
    )
```

```python
import jax
import jax.numpy as jnp
import numpy as np
from jax import lax
from jax.experimental import pallas as pl
from jax.experimental.pallas import tpu as pltpu
from jax.sharding import PartitionSpec as P

MESH = pl.DeviceIdType.MESH
HEADS = 4
DK = 128
D = 2048
BLOCK = 128
LENGTH = 1024
HALF = 512
EPS = 1e-6
C = 23
COLS = 256
LAG = 3
READY = 5 * LAG
OUT_C = 4
GU_C = 6
DOWN_C = 17
FFC = 11
F32 = jnp.float32
BF16 = jnp.bfloat16


def place():
    rep = lax.axis_index("rep")
    fs = lax.axis_index("fs")
    tp = lax.axis_index("tp")
    zl, y, x = fs // 16, (fs // 4) % 4, fs % 4
    z = rep * 2 + zl

    def dev(z_, y_, x_):
        return (z_ // 2, (z_ % 2) * 16 + y_ * 4 + x_, tp)

    xp, xm, yp, ym = (x + 1) % 4, (x + 3) % 4, (y + 1) % 4, (y + 3) % 4
    zp, zm = (z + 1) % 4, (z + 3) % 4
    to = dict(
        xp=dev(z, y, xp), xm=dev(z, y, xm), yp=dev(z, yp, x), ym=dev(z, ym, x), zp=dev(zp, y, x), zm=dev(zm, y, x)
    )
    return zl, y, x, xp, xm, yp, ym, to, (rep, fs, 1 - tp), tp


def wait_for(ref, sem):
    pltpu.make_async_copy(ref, ref, sem).wait()


def make_comm(W, send_sem, recv_sem, where):
    zl, y, x, xp, xm, yp, ym, to, partner, tp = where
    s0, s1, s2, s3 = (pl.ds(16 * i, 16) for i in range(4))
    lo, hi, al = pl.ds(0, 2), pl.ds(2, 2), slice(None)

    def put(c, stage, group, idx, d):
        r = W.at[(c,) + idx]
        pltpu.make_async_remote_copy(
            src_ref=r,
            dst_ref=r,
            send_sem=send_sem.at[group],
            recv_sem=recv_sem.at[c, stage],
            device_id=to[d],
            device_id_type=MESH,
        ).start()

    def send(c, s):
        if s == 0:
            for d in ("xp", "xm"):
                put(c, 0, 0, (zl, y, x, pl.ds(0, 32)), d)
            for d in ("yp", "ym"):
                put(c, 0, 0, (zl, y, x, pl.ds(32, 32)), d)
        elif s == 1:
            put(c, 1, 1, (zl, y, xm, s0), "xp")
            put(c, 1, 1, (zl, y, xp, s1), "xm")
            put(c, 1, 1, (zl, ym, x, s2), "yp")
            put(c, 1, 1, (zl, yp, x, s3), "ym")
        elif s == 2:
            for d in ("yp", "ym"):
                put(c, 2, 2, (zl, y, al, s0), d)
            for d in ("xp", "xm"):
                put(c, 2, 2, (zl, al, x, s2), d)
            put(c, 2, 2, (zl, y, lo, s1), "zp")
            put(c, 2, 2, (zl, y, hi, s1), "zm")
            put(c, 2, 2, (zl, lo, x, s3), "zp")
            put(c, 2, 2, (zl, hi, x, s3), "zm")
        elif s == 3:
            for d in ("yp", "ym"):
                put(c, 3, 4, (al, y, al, s1), d)
            for d in ("xp", "xm"):
                put(c, 3, 4, (al, al, x, s3), d)
            put(c, 3, 3, (zl, ym, lo, s0), "yp")
            put(c, 3, 3, (zl, yp, hi, s0), "ym")
            put(c, 3, 3, (zl, lo, xm, s2), "xp")
            put(c, 3, 3, (zl, hi, xp, s2), "xm")
        elif s == 4:
            put(c, 4, 5, (zl, lo, al, s0), "zp")
            put(c, 4, 5, (zl, hi, al, s0), "zm")
            put(c, 4, 5, (zl, al, lo, s2), "zp")
            put(c, 4, 5, (zl, al, hi, s2), "zm")
            put(c, 4, 5, (0, ym, al, s1), "yp")
            put(c, 4, 5, (1, yp, al, s1), "ym")
            put(c, 4, 5, (0, al, xm, s3), "xp")
            put(c, 4, 5, (1, al, xp, s3), "xm")

    three, two = pl.ds(0, 3), pl.ds(0, 2)

    def arrived(c, s):
        r = [
            W.at[c, 0, 0, two],
            W.at[c, 0, 0, 0],
            W.at[c, 0, three, two],
            W.at[pl.ds(0, 5), 0, 0, two],
            W.at[c, 0, three],
        ][s]
        wait_for(r, recv_sem.at[c, s])

    def drain():
        sizes = [W.at[:, 0, 0, two], W.at[:, 0, 0, 0], W.at[:, 0, three, two], W.at[:, 0, 0, two], W.at[:, :, 0], W.at[:, 0, three]]
        for i, r in enumerate(sizes):
            wait_for(r, send_sem.at[i])

    def tick(t):
        for s in range(6):
            c = t - LAG * s

            @pl.when((c >= 0) & (c < C))
            def _():
                if s:
                    arrived(c, s - 1)
                if s < 5:
                    send(c, s)

    return tick, drain


def nt(a, b):
    return lax.dot_general(a, b, (((1,), (1,)), ((), ())), preferred_element_type=F32)


def rows_normed(v, gain):
    return (v * lax.rsqrt(jnp.mean(v * v, axis=-1, keepdims=True) + EPS) * gain).astype(BF16)


def layer(
    src, tokens, mix_gain, ffn_gain, taps, cos, sin,
    out,
    W, xn, qs, ks, vs, dec, carry, hidden, mixs, mixr, pre, act, acc,
    send_sem, recv_sem, xsem, lsem,
):
    where = place()
    zl, y, x, to, partner, tp = where[0], where[1], where[2], where[7], where[8], where[9]
    other = 1 - tp
    tick, drain = make_comm(W, send_sem, recv_sem, where)
    own = pltpu.make_async_copy(src, W.at[:, zl, y, x], lsem)
    own.start()
    barrier = pltpu.get_barrier_semaphore()
    for d in list(to.values()) + [partner]:
        pl.semaphore_signal(barrier, inc=1, device_id=d, device_id_type=MESH)
    pl.semaphore_wait(barrier, 7)
    own.wait()

    def hand(src_ref, dst_ref, k):
        pltpu.make_async_remote_copy(
            src_ref=src_ref, dst_ref=dst_ref, send_sem=xsem.at[k], recv_sem=xsem.at[k + 1],
            device_id=partner, device_id_type=MESH,
        ).start()

    def rows_of(i):
        return pl.ds(pl.multiple_of(i * 128, 128), 128)

    def cols_of(n):
        return pl.ds(pl.multiple_of(n * 256, 256), 256)

    def hand_rows(i, k):
        r = xn.at[tp, rows_of(i)]
        hand(r, r, k)

    def norm_own(i):
        def one(k, _):
            r = pl.ds(pl.multiple_of(i * 128 + k * 32, 32), 32)
            xn[tp, r, :] = rows_normed(tokens[r, :].astype(F32), mix_gain[...])
            return 0

        lax.fori_loop(0, 4, one, 0)

    def tables():
        place_i = lax.broadcasted_iota(jnp.int32, (128, 128), 0).astype(F32)
        place_m = lax.broadcasted_iota(jnp.int32, (128, 128), 1).astype(F32)
        for h in range(2):
            g = jnp.full((128, 128), (tp * 2 + h).astype(F32))
            rate = (1.0 / 16.0) * jnp.exp(g * (np.log(32.0 / LENGTH) / (HEADS - 1)).astype(np.float32))
            gap = place_i - place_m
            dec[h, 0] = jnp.where(gap >= 0, jnp.exp(-jnp.maximum(gap, 0.0) * rate), 0.0)
            dec[h, 1] = jnp.exp(-(127.0 - place_i) * rate)
            dec[h, 2] = jnp.exp(-(place_i + 1.0) * rate)
            dec[h, 3] = jnp.exp(-128.0 * rate)
        pre[0:8, :] = jnp.zeros((8, 256), F32)

    def project(c, half):
        return jnp.dot(xn[half], W[c].reshape(2048, 256), preferred_element_type=F32)

    def qk_step(h):
        def one(half, _):
            u = project(2 * h, half).astype(BF16).astype(F32)
            r = pl.ds(pl.multiple_of(half * HALF, HALF), HALF)
            cs, sn = cos[r, :], sin[r, :]
            q, k = u[:, :128], u[:, 128:]
            qs[r, :] = (q * cs + pltpu.roll(q, 64, 1) * sn).astype(BF16)
            ks[r, :] = ((k * cs + pltpu.roll(k, 64, 1) * sn) * DK ** (-0.5)).astype(BF16)
            return 0

        lax.fori_loop(0, 2, one, 0)

    def v_step(h):
        def one(half, _):
            vs[pl.ds(pl.multiple_of(half * HALF, HALF), HALF), :] = project(2 * h + 1, half).astype(BF16)
            return 0

        lax.fori_loop(0, 2, one, 0)

    def retain(h):
        onset = jnp.concatenate([dec[h, 2]] * 2, axis=1)
        passing = jnp.concatenate([dec[h, 3]] * 2, axis=1)
        state = jnp.zeros((128, 256), F32)
        for b in range(8):
            r = slice(b * 128, b * 128 + 128)
            q, k, v = qs[r, :], ks[r, :], vs[r, :]
            weights = (nt(q, k) * dec[h, 0]).astype(BF16)
            ret = jnp.dot(weights, v, preferred_element_type=F32)
            if b:
                ret = ret + jnp.dot(q, state.astype(BF16), preferred_element_type=F32) * onset
            if b < 7:
                kd = (k.astype(F32) * dec[h, 1]).astype(BF16)
                fresh = lax.dot_general(kd, v, (((0,), (0,)), ((), ())), preferred_element_type=F32)
                state = state * passing + fresh if b else fresh
            cen = ret - jnp.mean(ret, axis=-1, keepdims=True)
            hidden[h, r, :] = (cen * lax.rsqrt(jnp.mean(cen * cen, axis=-1, keepdims=True) + EPS)).astype(BF16)

    def tile(c, n):
        return W[c, n // 4, n % 4].reshape(256, 256)

    def out_rows(half, n):
        r = pl.ds(pl.multiple_of(half * HALF, HALF), HALF)
        return nt(hidden[0, r, :], tile(OUT_C, n)) + nt(hidden[1, r, :], tile(OUT_C + 1, n))

    def send_cols(n, k):
        hand(mixs.at[:, cols_of(n)], mixr.at[:, cols_of(n)], k)

    def out_partner():
        def one(n, _):
            mixs[:, cols_of(n)] = out_rows(other, n).astype(BF16)

            @pl.when(n > 0)
            def _():
                send_cols(n - 1, 2)

            return 0

        lax.fori_loop(0, 8, one, 0)

    def out_own():
        def one(n, _):
            acc[0, :, cols_of(n)] = out_rows(tp, n).astype(BF16).astype(F32)

            @pl.when(n == 0)
            def _():
                send_cols(7, 2)

            return 0

        lax.fori_loop(0, 8, one, 0)

    def middle():
        wait_for(xn.at[0], xsem.at[0])
        wait_for(mixr, xsem.at[3])

        def one(i, _):
            for k in range(4):
                r = pl.ds(pl.multiple_of(i * 128 + k * 32, 32), 32)
                resid = (tokens[r, :].astype(F32) + (acc[0, r, :] + mixr[r, :].astype(F32))).astype(BF16)
                out[r, :] = resid
                xn[tp, r, :] = rows_normed(resid.astype(F32), ffn_gain[...])

            @pl.when(i > 0)
            def _():
                hand_rows(i - 1, 4)

            return 0

        lax.fori_loop(0, 4, one, 0)

    def gu_half(j, half):
        r = pl.ds(pl.multiple_of(8 + half * HALF, 8), HALF)
        pre[r, :] = project(GU_C + j, half).astype(BF16).astype(F32)

    def gu_step(j):
        gu_half(j, tp)

        @pl.when(j == 0)
        def _():
            hand_rows(3, 4)
            wait_for(xn.at[0], xsem.at[5])

        gu_half(j, other)
        k0, k1, k2 = taps[j, 0:1, :], taps[j, 1:2, :], taps[j, 2:3, :]
        lane = pl.ds(pl.multiple_of((j % 2) * 128, 128), 128)

        def one(i, _):
            u = pre[pl.ds(pl.multiple_of(i * 128, 128), 136), :]
            conv = k0 * pltpu.roll(u, 2, 0) + k1 * pltpu.roll(u, 1, 0) + k2 * u
            g, w = conv[8:, :128], conv[8:, 128:]
            act[j // 2, i // 4, pl.ds(pl.multiple_of((i % 4) * 128, 128), 128), lane] = (
                g / (1.0 + jnp.exp(-g)) * w
            ).astype(BF16)
            return 0

        lax.fori_loop(0, 8, one, 0)

    def down_first():
        def one(n, _):
            ws = [tile(DOWN_C + i, n) for i in range(4)]
            for half in range(2):
                o = nt(act[0, half], ws[0])
                for i in range(1, 4):
                    o = o + nt(act[i, half], ws[i])
                acc[half, :, cols_of(n)] = o
            return 0

        lax.fori_loop(0, 8, one, 0)

    def down_rows(half, n):
        o = acc[half, :, cols_of(n)] + nt(act[4, half], tile(DOWN_C + 4, n))
        return (o + nt(act[5, half, :, :128], tile(DOWN_C + 5, n)[:, :128])).astype(BF16)

    def down_last():
        wait_for(mixs, xsem.at[2])

        def one(n, _):
            mixs[:, cols_of(n)] = down_rows(other, n)

            @pl.when(n > 0)
            def _():
                send_cols(n - 1, 6)

            return 0

        lax.fori_loop(0, 8, one, 0)

        def two(n, _):
            acc[tp, :, cols_of(n)] = down_rows(tp, n).astype(F32)

            @pl.when(n == 0)
            def _():
                send_cols(7, 6)

            return 0

        lax.fori_loop(0, 8, two, 0)
        wait_for(mixr, xsem.at[7])

        def fin(i, _):
            r = pl.ds(pl.multiple_of(i * 32, 32), 32)
            out[r, :] = (out[r, :].astype(F32) + (acc[tp, r, :] + mixr[r, :].astype(F32))).astype(BF16)
            return 0

        lax.fori_loop(0, 16, fin, 0)
        wait_for(xn.at[0], xsem.at[4])
        wait_for(mixs, xsem.at[6])

    GU0 = READY + GU_C + 2
    LAST = READY + C - 1

    def step(t, _):
        tick(t)

        @pl.when((t >= 3) & (t < 7))
        def _():
            norm_own(t - 3)

        @pl.when((t >= 4) & (t < 8))
        def _():
            hand_rows(t - 4, 0)

        @pl.when(t == 8)
        def _():
            tables()

        @pl.when(t == READY)
        def _():
            wait_for(xn.at[0], xsem.at[1])

        @pl.when((t == READY) | (t == READY + 2))
        def _():
            qk_step((t - READY) // 2)

        @pl.when((t == READY + 1) | (t == READY + 3))
        def _():
            h = (t - READY - 1) // 2
            v_step(h)
            retain(h)

        @pl.when(t == READY + 5)
        def _():
            out_partner()

        @pl.when(t == READY + 6)
        def _():
            out_own()

        @pl.when(t == READY + 7)
        def _():
            middle()

        @pl.when((t >= GU0) & (t < GU0 + 9 + 0))
        def _():
            first = jnp.where(t < GU0 + 2, 2 * (t - GU0), t - READY - GU_C)
            count = jnp.where(t < GU0 + 2, 2, 1)
            lax.fori_loop(first, first + count, lambda j, _: (gu_step(j), 0)[1], 0)

        @pl.when(t == LAST - 2)
        def _():
            down_first()

        @pl.when(t == LAST)
        def _():
            down_last()

        return 0

    lax.fori_loop(0, LAST + 1, step, 0)
    drain()


def own_chunks(w_query, w_key, w_value, w_out, w_ffgate, w_ffup, w_down):
    parts = []
    for h in range(2):
        parts += [w_query[:, h * 128 : h * 128 + 128], w_key[:, h * 128 : h * 128 + 128]]
        parts.append(w_value[:, h * 256 : h * 256 + 256])
    parts.append(w_out.T)
    for j in range(FFC):
        parts += [w_ffgate[:, j * 128 : j * 128 + 128], w_ffup[:, j * 128 : j * 128 + 128]]
    parts += [w_down.T, jnp.zeros((64, 128), BF16)]
    flat = jnp.concatenate(parts, axis=1)
    return jnp.transpose(flat.reshape(64, C, COLS), (1, 0, 2))


def angle_tables():
    inverse = 10000.0 ** (-np.arange(64) * 2.0 / 128)
    angles = np.arange(LENGTH)[:, None] * inverse[None, :]
    cos, sin = np.cos(angles), np.sin(angles)
    return (
        np.concatenate([cos, cos], axis=1).astype(np.float32),
        np.concatenate([-sin, sin], axis=1).astype(np.float32),
    )


def body(
    tokens, mix_gain, w_query, w_key, w_value, w_out, ffn_gain, w_ffgate, w_ffup, conv_gate, conv_up, w_down
):
    tp = lax.axis_index("tp")
    src = own_chunks(w_query, w_key, w_value, w_out, w_ffgate, w_ffup, w_down)
    ff = FFC * 128
    taps = [lax.dynamic_slice_in_dim(a, tp * ff, ff, 1).reshape(3, FFC, 128) for a in (conv_gate, conv_up)]
    taps = jnp.transpose(jnp.concatenate(taps, axis=2), (1, 0, 2))
    cos, sin = angle_tables()
    vmem = pl.BlockSpec(memory_space=pltpu.VMEM)
    return pl.pallas_call(
        layer,
        out_shape=jax.ShapeDtypeStruct((HALF, D), BF16),
        in_specs=[pl.BlockSpec(memory_space=pl.ANY)] + [vmem] * 6,
        out_specs=vmem,
        scratch_shapes=[
            pltpu.VMEM((C, 2, 4, 4, 64, COLS), BF16),
            pltpu.VMEM((2, HALF, D), BF16),
            pltpu.VMEM((LENGTH, 128), BF16),
            pltpu.VMEM((LENGTH, 128), BF16),
            pltpu.VMEM((LENGTH, 256), BF16),
            pltpu.VMEM((2, 4, 128, 128), F32),
            pltpu.VMEM((8, 128), F32),
            pltpu.VMEM((2, LENGTH, 256), BF16),
            pltpu.VMEM((HALF, D), BF16),
            pltpu.VMEM((HALF, D), BF16),
            pltpu.VMEM((8 + LENGTH, 256), F32),
            pltpu.VMEM((6, 2, HALF, 256), BF16),
            pltpu.VMEM((2, HALF, D), F32),
            pltpu.SemaphoreType.DMA((6,)),
            pltpu.SemaphoreType.DMA((C, 5)),
            pltpu.SemaphoreType.DMA((8,)),
            pltpu.SemaphoreType.DMA,
        ],
        compiler_params=pltpu.CompilerParams(
            collective_id=0, has_side_effects=True, vmem_limit_bytes=67043328
        ),
    )(src, tokens, mix_gain.reshape(1, D), ffn_gain.reshape(1, D), taps, jnp.asarray(cos), jnp.asarray(sin))


def solution(mesh):
    w = P("fs", "tp")
    placed = (P(("rep", "fs", "tp"), None), P(), w, w, w, P("tp", "fs"), P(), w, w, P(), P(), P("tp", "fs"))
    return jax.shard_map(
        body, mesh=mesh, in_specs=placed, out_specs=P(("rep", "fs", "tp"), None), check_vma=False
    )
```

```python
import jax
import jax.numpy as jnp
import numpy as np
from jax import lax
from jax.experimental import pallas as pl
from jax.experimental.pallas import tpu as pltpu
from jax.sharding import PartitionSpec as P

MESH = pl.DeviceIdType.MESH
HEADS = 4
DK = 128
D = 2048
BLOCK = 128
LENGTH = 1024
HALF = 512
EPS = 1e-6
C = 23
COLS = 256
LAG = 3
READY = 3 * LAG
FULL = 22
VLIM = 67043328
NORM = 20
GROUPS = ((0, 2), (2, 6), (6, 14), (14, 22), (22, 23))
OUT_C = 4
GU_C = 6
DOWN_C = 17
FFC = 11
F32 = jnp.float32
BF16 = jnp.bfloat16


def place():
    rep = lax.axis_index("rep")
    fs = lax.axis_index("fs")
    tp = lax.axis_index("tp")
    zl, y, x = fs // 16, (fs // 4) % 4, fs % 4
    z = rep * 2 + zl

    def dev(z_, y_, x_):
        return (z_ // 2, (z_ % 2) * 16 + y_ * 4 + x_, tp)

    xp, xm, yp, ym = (x + 1) % 4, (x + 3) % 4, (y + 1) % 4, (y + 3) % 4
    zp, zm = (z + 1) % 4, (z + 3) % 4
    to = dict(
        xp=dev(z, y, xp), xm=dev(z, y, xm), yp=dev(z, yp, x), ym=dev(z, ym, x), zp=dev(zp, y, x), zm=dev(zm, y, x)
    )
    return zl, y, x, xp, xm, yp, ym, to, (rep, fs, 1 - tp), tp


def wait_for(ref, sem):
    pltpu.make_async_copy(ref, ref, sem).wait()


def make_comm(W, send_sem, recv_sem, early_sem, where):
    zl, y, x, xp, xm, yp, ym, to, partner, tp = where
    s0, s1, s2, s3 = (pl.ds(16 * i, 16) for i in range(4))
    lo, hi, al = pl.ds(0, 2), pl.ds(2, 2), slice(None)
    two, three = pl.ds(0, 2), pl.ds(0, 3)

    def put(r, sem, recv, d):
        pltpu.make_async_remote_copy(
            src_ref=r, dst_ref=r, send_sem=sem, recv_sem=recv, device_id=to[d], device_id_type=MESH
        ).start()

    def lanes_of(half):
        return pl.ds(0, 128) if half else pl.ds(0, 256)

    def early(g, s):
        c0, c1 = GROUPS[g]
        cs, lanes = pl.ds(c0, c1 - c0), lanes_of(c0 == FULL)
        sem, recv = early_sem.at[g, s], early_sem.at[g, 2 + s]
        if s == 0:
            for d in ("xp", "xm"):
                put(W.at[cs, zl, y, x, pl.ds(0, 32), lanes], sem, recv, d)
            for d in ("yp", "ym"):
                put(W.at[cs, zl, y, x, pl.ds(32, 32), lanes], sem, recv, d)
        else:
            put(W.at[cs, zl, y, xm, s0, lanes], sem, recv, "xp")
            put(W.at[cs, zl, y, xp, s1, lanes], sem, recv, "xm")
            put(W.at[cs, zl, ym, x, s2, lanes], sem, recv, "yp")
            put(W.at[cs, zl, yp, x, s3, lanes], sem, recv, "ym")

    def early_ref(g, s):
        c0, c1 = GROUPS[g]
        cs, lanes = pl.ds(c0, c1 - c0), lanes_of(c0 == FULL)
        return W.at[cs, 0, 0, two if s == 0 else pl.ds(0, 1), :, lanes]

    def early_arrived(g, s):
        wait_for(early_ref(g, s), early_sem.at[g, 2 + s])

    def send(c, s):
        def go(group, idx, d):
            put(W.at[(c,) + idx], send_sem.at[group], recv_sem.at[c, s - 2], d)

        if s == 2:
            for d in ("yp", "ym"):
                go(0, (zl, y, al, s0), d)
            for d in ("xp", "xm"):
                go(0, (zl, al, x, s2), d)
            go(0, (zl, y, lo, s1), "zp")
            go(0, (zl, y, hi, s1), "zm")
            go(0, (zl, lo, x, s3), "zp")
            go(0, (zl, hi, x, s3), "zm")
        elif s == 3:
            for d in ("yp", "ym"):
                go(2, (al, y, al, s1), d)
            for d in ("xp", "xm"):
                go(2, (al, al, x, s3), d)
            go(1, (zl, ym, lo, s0), "yp")
            go(1, (zl, yp, hi, s0), "ym")
            go(1, (zl, lo, xm, s2), "xp")
            go(1, (zl, hi, xp, s2), "xm")
        elif s == 4:
            go(3, (zl, lo, al, s0), "zp")
            go(3, (zl, hi, al, s0), "zm")
            go(3, (zl, al, lo, s2), "zp")
            go(3, (zl, al, hi, s2), "zm")
            go(3, (0, ym, al, s1), "yp")
            go(3, (1, yp, al, s1), "ym")
            go(3, (0, al, xm, s3), "xp")
            go(3, (1, al, xp, s3), "xm")

    top, low = pl.ds(0, 32), pl.ds(32, 32)

    def send_late(c, s, half):
        def go(idx, d):
            put(W.at[(c,) + idx + (lanes_of(half),)], send_sem.at[4 + 3 * half + s - 2], recv_sem.at[c, s - 2], d)

        if s == 2:
            go((zl, y, lo, top), "zp")
            go((zl, y, hi, top), "zm")
            go((zl, lo, x, low), "zp")
            go((zl, hi, x, low), "zm")
        elif s == 3:
            for d in ("yp", "ym"):
                go((al, y, al, top), d)
            for d in ("xp", "xm"):
                go((al, al, x, low), d)
        elif s == 4:
            go((0, ym, al, top), "yp")
            go((1, yp, al, top), "ym")
            go((0, al, xm, low), "xp")
            go((1, al, xp, low), "xm")

    def late_refs(cs, half):
        ln = lanes_of(half)
        return [W.at[cs, 0, 0, :, :, ln], W.at[cs, 0, :, :, :, ln], W.at[cs, :, 0, :, :, ln]]

    def arrived(c, s):
        r = [W.at[c, 0, three, two], W.at[pl.ds(0, 5), 0, 0, two], W.at[c, 0, three]][s - 2]
        wait_for(r, recv_sem.at[c, s - 2])

    def drain():
        for g in range(len(GROUPS)):
            for s in range(2):
                wait_for(early_ref(g, s), early_sem.at[g, s])
        cs = pl.ds(0, NORM)
        for i, r in enumerate([W.at[cs, 0, three, two], W.at[cs, 0, 0, two], W.at[cs, :, 0], W.at[cs, 0, three]]):
            wait_for(r, send_sem.at[i])
        for half in range(2):
            for i, r in enumerate(late_refs(pl.ds(FULL, 1) if half else pl.ds(NORM, FULL - NORM), half)):
                wait_for(r, send_sem.at[4 + 3 * half + i])

    def tick(t):
        for s in range(2, 6):
            c = t - LAG * (s - 2)

            @pl.when((c >= 0) & (c < NORM))
            def _():
                if s > 2:
                    arrived(c, s - 1)
                if s < 5:
                    send(c, s)

            def late(half):
                if s > 2:
                    wait_for(late_refs(c, half)[s - 3], recv_sem.at[c, s - 3])
                if s < 5:
                    send_late(c, s, half)

            @pl.when((c >= NORM) & (c < FULL))
            def _():
                late(0)

            @pl.when(c == FULL)
            def _():
                late(1)

    return tick, drain, early, early_arrived


def nt(a, b):
    return lax.dot_general(a, b, (((1,), (1,)), ((), ())), preferred_element_type=F32)


def rows_normed(v, gain):
    return (v * lax.rsqrt(jnp.mean(v * v, axis=-1, keepdims=True) + EPS) * gain).astype(BF16)


def layer(
    w_query, w_key, w_value, w_outt, w_ffgate, w_ffup, w_downt,
    tokens_in, cos_in, sin_in, mix_gain, ffn_gain, tap_gate, tap_up,
    out,
    W, tokens, cos, sin, xn, qs, ks, vs, dec, hidden, mixs, mixr, pre_a, pre_b, act, acc,
    send_sem, recv_sem, early_sem, xsem, lsem, fsem,
):
    where = place()
    zl, y, x, to, partner, tp = where[0], where[1], where[2], where[7], where[8], where[9]
    other = 1 - tp
    tick, drain, early, early_arrived = make_comm(W, send_sem, recv_sem, early_sem, where)

    def load(ref, c, lanes, g):
        pltpu.make_async_copy(ref, W.at[c, zl, y, x, :, lanes], lsem.at[g]).start()

    own_rows = [pltpu.make_async_copy(a, b, lsem.at[k]) for a, b, k in ((tokens_in, tokens, 5), (cos_in, cos, 6), (sin_in, sin, 7))]
    own_rows[0].start()
    left, right, whole = pl.ds(0, 128), pl.ds(128, 128), pl.ds(0, 256)
    for h in range(2):
        load(w_query.at[:, pl.ds(h * 128, 128)], 2 * h, left, h)
        load(w_key.at[:, pl.ds(h * 128, 128)], 2 * h, right, h)
        load(w_value.at[:, pl.ds(h * 256, 256)], 2 * h + 1, whole, h)
    for i in range(2):
        load(w_outt.at[:, pl.ds(i * 256, 256)], OUT_C + i, whole, 1)
    for j in range(FFC):
        g = 2 if GU_C + j < GROUPS[2][1] else 3
        load(w_ffgate.at[:, pl.ds(j * 128, 128)], GU_C + j, left, g)
        load(w_ffup.at[:, pl.ds(j * 128, 128)], GU_C + j, right, g)
    for i in range(5):
        load(w_downt.at[:, pl.ds(i * 256, 256)], DOWN_C + i, whole, 3)
    load(w_downt.at[:, pl.ds(1280, 128)], FULL, left, 4)
    own_rows[1].start()
    own_rows[2].start()

    def loaded(g):
        c0, c1 = GROUPS[g]
        wait_for(W.at[pl.ds(c0, c1 - c0), zl, y, x, :, left if g == 4 else whole], lsem.at[g])

    barrier = pltpu.get_barrier_semaphore()
    for d in list(to.values()) + [partner]:
        pl.semaphore_signal(barrier, inc=1, device_id=d, device_id_type=MESH)
    pl.semaphore_wait(barrier, 7)

    def hand(src_ref, dst_ref, k):
        pltpu.make_async_remote_copy(
            src_ref=src_ref, dst_ref=dst_ref, send_sem=xsem.at[k], recv_sem=xsem.at[k + 1],
            device_id=partner, device_id_type=MESH,
        ).start()

    def rows_of(i):
        return pl.ds(pl.multiple_of(i * 128, 128), 128)

    def cols_of(n):
        return pl.ds(pl.multiple_of(n * 256, 256), 256)

    def hand_rows(i, k):
        r = xn.at[tp, rows_of(i)]
        hand(r, r, k)

    def norm_own(i):
        def one(k, _):
            r = pl.ds(pl.multiple_of(i * 128 + k * 32, 32), 32)
            xn[tp, r, :] = rows_normed(tokens[r, :].astype(F32), mix_gain[...])
            return 0

        lax.fori_loop(0, 4, one, 0)

    def tables():
        place_i = lax.broadcasted_iota(jnp.int32, (128, 128), 0).astype(F32)
        place_m = lax.broadcasted_iota(jnp.int32, (128, 128), 1).astype(F32)
        for h in range(2):
            g = jnp.full((128, 128), (tp * 2 + h).astype(F32))
            rate = (1.0 / 16.0) * jnp.exp(g * (np.log(32.0 / LENGTH) / (HEADS - 1)).astype(np.float32))
            gap = place_i - place_m
            dec[h, 0] = jnp.where(gap >= 0, jnp.exp(-jnp.maximum(gap, 0.0) * rate), 0.0)
            dec[h, 1] = jnp.exp(-(127.0 - place_i) * rate)
            dec[h, 2] = jnp.exp(-(place_i + 1.0) * rate)
            dec[h, 3] = jnp.exp(-128.0 * rate)
        pre_a[0:8, :] = jnp.zeros((8, 256), F32)

        def clear(i, _):
            pre_b[pl.ds(pl.multiple_of(i * 8, 8), 8), :] = jnp.zeros((8, 256), F32)
            return 0

        lax.fori_loop(0, (8 + LENGTH) // 8, clear, 0)

    def project(c, half):
        return jnp.dot(xn[half], W[c].reshape(2048, 256), preferred_element_type=F32)

    def qk_step(h):
        def one(half, _):
            u = project(2 * h, half).astype(BF16).astype(F32)
            r = pl.ds(pl.multiple_of(half * HALF, HALF), HALF)
            cs, sn = cos[r, :], sin[r, :]
            q, k = u[:, :128], u[:, 128:]
            qs[r, :] = (q * cs + pltpu.roll(q, 64, 1) * sn).astype(BF16)
            ks[r, :] = ((k * cs + pltpu.roll(k, 64, 1) * sn) * DK ** (-0.5)).astype(BF16)
            return 0

        lax.fori_loop(0, 2, one, 0)

    def v_step(h):
        def one(half, _):
            vs[pl.ds(pl.multiple_of(half * HALF, HALF), HALF), :] = project(2 * h + 1, half).astype(BF16)
            return 0

        lax.fori_loop(0, 2, one, 0)

    def retain(h):
        onset = jnp.concatenate([dec[h, 2]] * 2, axis=1)
        passing = jnp.concatenate([dec[h, 3]] * 2, axis=1)
        state = jnp.zeros((128, 256), F32)
        for b in range(8):
            r = slice(b * 128, b * 128 + 128)
            q, k, v = qs[r, :], ks[r, :], vs[r, :]
            weights = (nt(q, k) * dec[h, 0]).astype(BF16)
            ret = jnp.dot(weights, v, preferred_element_type=F32)
            if b:
                ret = ret + jnp.dot(q, state.astype(BF16), preferred_element_type=F32) * onset
            if b < 7:
                kd = (k.astype(F32) * dec[h, 1]).astype(BF16)
                fresh = lax.dot_general(kd, v, (((0,), (0,)), ((), ())), preferred_element_type=F32)
                state = state * passing + fresh if b else fresh
            cen = ret - jnp.mean(ret, axis=-1, keepdims=True)
            hidden[h, r, :] = (cen * lax.rsqrt(jnp.mean(cen * cen, axis=-1, keepdims=True) + EPS)).astype(BF16)

    def tile(c, n):
        return W[c, n // 4, n % 4].reshape(256, 256)

    def out_rows(half, n):
        r = pl.ds(pl.multiple_of(half * HALF, HALF), HALF)
        return nt(hidden[0, r, :], tile(OUT_C, n)) + nt(hidden[1, r, :], tile(OUT_C + 1, n))

    def send_cols(n, k):
        hand(mixs.at[:, cols_of(n)], mixr.at[:, cols_of(n)], k)

    def out_partner():
        def one(n, _):
            mixs[:, cols_of(n)] = out_rows(other, n).astype(BF16)

            @pl.when(n > 0)
            def _():
                send_cols(n - 1, 2)

            return 0

        lax.fori_loop(0, 8, one, 0)

    def out_own():
        def one(n, _):
            acc[0, :, cols_of(n)] = out_rows(tp, n).astype(BF16).astype(F32)

            @pl.when(n == 0)
            def _():
                send_cols(7, 2)

            return 0

        lax.fori_loop(0, 8, one, 0)

    def middle():
        wait_for(xn.at[0], xsem.at[0])
        wait_for(mixr, xsem.at[3])

        def one(i, _):
            for k in range(4):
                r = pl.ds(pl.multiple_of(i * 128 + k * 32, 32), 32)
                resid = (tokens[r, :].astype(F32) + (acc[0, r, :] + mixr[r, :].astype(F32))).astype(BF16)
                out[r, :] = resid
                xn[tp, r, :] = rows_normed(resid.astype(F32), ffn_gain[...])

            @pl.when(i > 0)
            def _():
                hand_rows(i - 1, 4)

            return 0

        lax.fori_loop(0, 4, one, 0)

    def gu_dot(j, half, pre):
        r = pl.ds(pl.multiple_of(8 + half * HALF, 8), HALF)
        pre[r, :] = project(GU_C + j, half).astype(BF16).astype(F32)

    def gu_conv(j, half, pre):
        mine = pl.ds(pl.multiple_of(tp * (FFC * 128) + j * 128, 128), 128)
        k0, k1, k2 = (
            jnp.concatenate([tap_gate[k : k + 1, mine], tap_up[k : k + 1, mine]], axis=1) for k in range(3)
        )
        lane = pl.ds(pl.multiple_of((j % 2) * 128, 128), 128)
        for i in range(8):
            u = pre[pl.ds(pl.multiple_of(half * HALF + i * 64, 64), 72), :]
            conv = k0 * pltpu.roll(u, 2, 0) + k1 * pltpu.roll(u, 1, 0) + k2 * u
            g, w = conv[8:, :128], conv[8:, 128:]
            act[j // 2, half, i * 64 : i * 64 + 64, lane] = (g / (1.0 + jnp.exp(-g)) * w).astype(BF16)

    def gu_step(j, now, before):
        last = jnp.maximum(j - 1, 0)
        gu_dot(j, tp, now)
        gu_conv(last, tp, before)

        @pl.when(j == 0)
        def _():
            hand_rows(3, 4)
            wait_for(xn.at[0], xsem.at[5])

        gu_dot(j, other, now)
        gu_conv(last, other, before)

    def down_first(n0):
        def one(n, _):
            ws = [tile(DOWN_C + i, n) for i in range(4)]
            for half in range(2):
                o = nt(act[0, half], ws[0])
                for i in range(1, 4):
                    o = o + nt(act[i, half], ws[i])
                acc[half, :, cols_of(n)] = o
            return 0

        lax.fori_loop(n0, n0 + 4, one, 0)

    def down_rows(half, n):
        o = acc[half, :, cols_of(n)] + nt(act[4, half], tile(DOWN_C + 4, n))
        return (o + nt(act[5, half, :, :128], tile(DOWN_C + 5, n)[:, :128])).astype(BF16)

    def send_piece(n):
        pltpu.make_async_remote_copy(
            src_ref=mixs.at[:, cols_of(n)], dst_ref=mixr.at[:, cols_of(n)], send_sem=xsem.at[6], recv_sem=fsem.at[n],
            device_id=partner, device_id_type=MESH,
        ).start()

    def down_last():
        wait_for(mixs, xsem.at[2])

        def one(n, _):
            mixs[:, cols_of(n)] = down_rows(other, n)

            @pl.when(n > 0)
            def _():
                send_piece(n - 1)

            return 0

        lax.fori_loop(0, 8, one, 0)

        def two(n, _):
            mine = down_rows(tp, n).astype(F32)

            @pl.when(n == 0)
            def _():
                send_piece(7)

            wait_for(mixr.at[:, pl.ds(0, 256)], fsem.at[n])
            out[:, cols_of(n)] = (
                out[:, cols_of(n)].astype(F32) + (mine + mixr[:, cols_of(n)].astype(F32))
            ).astype(BF16)
            return 0

        lax.fori_loop(0, 8, two, 0)
        wait_for(xn.at[0], xsem.at[4])
        wait_for(mixs, xsem.at[6])

    GU0 = READY + GU_C + 2
    NORM0 = READY - 5
    LAST = READY + C - 1

    loaded(0)
    early(0, 0)
    loaded(1)
    early(1, 0)
    early_arrived(0, 0)
    early(0, 1)
    loaded(2)
    early(2, 0)
    early_arrived(1, 0)
    early(1, 1)

    def step(t, _):
        for g in (0, 1, 2, 3, 4):
            @pl.when(t == GROUPS[g][0])
            def _():
                early_arrived(g, 1)

        tick(t)

        @pl.when(t == 1)
        def _():
            for g in (3, 4):
                loaded(g)
                early(g, 0)

        @pl.when(t == 2)
        def _():
            early_arrived(2, 0)
            early(2, 1)

        @pl.when(t == 4)
        def _():
            for g in (3, 4):
                early_arrived(g, 0)
                early(g, 1)

        @pl.when(t == NORM0)
        def _():
            own_rows[0].wait()

        @pl.when((t >= NORM0) & (t < NORM0 + 4))
        def _():
            norm_own(t - NORM0)

        @pl.when((t > NORM0) & (t <= NORM0 + 4))
        def _():
            hand_rows(t - NORM0 - 1, 0)

        @pl.when(t == NORM0 - 1)
        def _():
            tables()

        @pl.when(t == READY)
        def _():
            own_rows[1].wait()
            own_rows[2].wait()
            wait_for(xn.at[0], xsem.at[1])

        @pl.when((t == READY) | (t == READY + 2))
        def _():
            qk_step((t - READY) // 2)

        @pl.when((t == READY + 1) | (t == READY + 3))
        def _():
            v_step((t - READY - 1) // 2)

        @pl.when((t == READY + 1) | (t == READY + 4))
        def _():
            retain((t - READY - 1) // 3)

        @pl.when(t == READY + 5)
        def _():
            out_partner()

        @pl.when(t == READY + 6)
        def _():
            out_own()

        @pl.when(t == READY + 7)
        def _():
            middle()

        @pl.when((t >= GU0) & (t < GU0 + FFC) & ((t - GU0) % 2 == 0))
        def _():
            gu_step(t - GU0, pre_a, pre_b)

        @pl.when((t >= GU0) & (t < GU0 + FFC) & ((t - GU0) % 2 == 1))
        def _():
            gu_step(t - GU0, pre_b, pre_a)

        @pl.when(t == GU0 + FFC)
        def _():
            lax.fori_loop(0, 2, lambda half, _: (gu_conv(FFC - 1, half, pre_a), 0)[1], 0)

        @pl.when((t == LAST - 2) | (t == LAST - 1))
        def _():
            down_first(4 * (t - LAST + 2))

        @pl.when(t == LAST)
        def _():
            down_last()

        return 0

    lax.fori_loop(0, LAST + 1, step, 0)
    drain()


def angle_tables():
    inverse = 10000.0 ** (-np.arange(64) * 2.0 / 128)
    angles = np.arange(LENGTH)[:, None] * inverse[None, :]
    cos, sin = np.cos(angles), np.sin(angles)
    return (
        np.concatenate([cos, cos], axis=1).astype(np.float32),
        np.concatenate([-sin, sin], axis=1).astype(np.float32),
    )


def body(
    tokens, mix_gain, w_query, w_key, w_value, w_out, ffn_gain, w_ffgate, w_ffup, conv_gate, conv_up, w_down
):
    cos, sin = angle_tables()
    vmem = pl.BlockSpec(memory_space=pltpu.VMEM)
    hbm = pl.BlockSpec(memory_space=pl.ANY)
    whole = jax.ShapeDtypeStruct((HALF, D), BF16)
    return pl.pallas_call(
        layer,
        out_shape=whole,
        in_specs=[hbm] * 10 + [vmem] * 4,
        out_specs=vmem,
        scratch_shapes=[
            pltpu.VMEM((C, 2, 4, 4, 64, COLS), BF16),
            pltpu.VMEM((HALF, D), BF16),
            pltpu.VMEM((LENGTH, 128), F32),
            pltpu.VMEM((LENGTH, 128), F32),
            pltpu.VMEM((2, HALF, D), BF16),
            pltpu.VMEM((LENGTH, 128), BF16),
            pltpu.VMEM((LENGTH, 128), BF16),
            pltpu.VMEM((LENGTH, 256), BF16),
            pltpu.VMEM((2, 4, 128, 128), F32),
            pltpu.VMEM((2, LENGTH, 256), BF16),
            pltpu.VMEM((HALF, D), BF16),
            pltpu.VMEM((HALF, D), BF16),
            pltpu.VMEM((8 + LENGTH, 256), F32),
            pltpu.VMEM((8 + LENGTH, 256), F32),
            pltpu.VMEM((6, 2, HALF, 256), BF16),
            pltpu.VMEM((2, HALF, D), F32),
            pltpu.SemaphoreType.DMA((10,)),
            pltpu.SemaphoreType.DMA((C, 3)),
            pltpu.SemaphoreType.DMA((len(GROUPS), 4)),
            pltpu.SemaphoreType.DMA((8,)),
            pltpu.SemaphoreType.DMA((8,)),
            pltpu.SemaphoreType.DMA((8,)),
        ],
        compiler_params=pltpu.CompilerParams(
            collective_id=0, has_side_effects=True, vmem_limit_bytes=VLIM
        ),
    )(
        w_query, w_key, w_value, w_out.T, w_ffgate, w_ffup, w_down.T,
        tokens, jnp.asarray(cos), jnp.asarray(sin), mix_gain.reshape(1, D), ffn_gain.reshape(1, D), conv_gate, conv_up,
    )


def solution(mesh):
    w = P("fs", "tp")
    placed = (P(("rep", "fs", "tp"), None), P(), w, w, w, P("tp", "fs"), P(), w, w, P(), P(), P("tp", "fs"))
    return jax.shard_map(
        body, mesh=mesh, in_specs=placed, out_specs=P(("rep", "fs", "tp"), None), check_vma=False
    )
```

```python
import jax
import jax.numpy as jnp
import numpy as np
from jax import lax
from jax.experimental import pallas as pl
from jax.experimental.pallas import tpu as pltpu
from jax.sharding import PartitionSpec as P

MESH = pl.DeviceIdType.MESH
HEADS = 4
DK = 128
D = 2048
BLOCK = 128
LENGTH = 1024
HALF = 512
EPS = 1e-6
C = 23
COLS = 256
LAG = 3
READY = 3 * LAG
FULL = 22
VLIM = 67043328
NORM = 20
GROUPS = ((0, 2), (2, 6), (6, 14), (14, 22), (22, 23))
OUT_C = 4
GU_C = 6
DOWN_C = 17
FFC = 11
F32 = jnp.float32
BF16 = jnp.bfloat16


def place():
    rep = lax.axis_index("rep")
    fs = lax.axis_index("fs")
    tp = lax.axis_index("tp")
    zl, y, x = fs // 16, (fs // 4) % 4, fs % 4
    z = rep * 2 + zl

    def dev(z_, y_, x_):
        return (z_ // 2, (z_ % 2) * 16 + y_ * 4 + x_, tp)

    xp, xm, yp, ym = (x + 1) % 4, (x + 3) % 4, (y + 1) % 4, (y + 3) % 4
    zp, zm = (z + 1) % 4, (z + 3) % 4
    to = dict(
        xp=dev(z, y, xp), xm=dev(z, y, xm), yp=dev(z, yp, x), ym=dev(z, ym, x), zp=dev(zp, y, x), zm=dev(zm, y, x)
    )
    return zl, y, x, xp, xm, yp, ym, to, (rep, fs, 1 - tp), tp


def wait_for(ref, sem):
    pltpu.make_async_copy(ref, ref, sem).wait()


def make_comm(W, send_sem, recv_sem, early_sem, where):
    zl, y, x, xp, xm, yp, ym, to, partner, tp = where
    s0, s1, s2, s3 = (pl.ds(16 * i, 16) for i in range(4))
    lo, hi, al = pl.ds(0, 2), pl.ds(2, 2), slice(None)
    two, three = pl.ds(0, 2), pl.ds(0, 3)

    def put(r, sem, recv, d):
        pltpu.make_async_remote_copy(
            src_ref=r, dst_ref=r, send_sem=sem, recv_sem=recv, device_id=to[d], device_id_type=MESH
        ).start()

    def lanes_of(half):
        return pl.ds(0, 128) if half else pl.ds(0, 256)

    def early(g, s):
        c0, c1 = GROUPS[g]
        cs, lanes = pl.ds(c0, c1 - c0), lanes_of(c0 == FULL)
        sem, recv = early_sem.at[g, s], early_sem.at[g, 2 + s]
        if s == 0:
            for d in ("xp", "xm"):
                put(W.at[cs, zl, y, x, pl.ds(0, 32), lanes], sem, recv, d)
            for d in ("yp", "ym"):
                put(W.at[cs, zl, y, x, pl.ds(32, 32), lanes], sem, recv, d)
        else:
            put(W.at[cs, zl, y, xm, s0, lanes], sem, recv, "xp")
            put(W.at[cs, zl, y, xp, s1, lanes], sem, recv, "xm")
            put(W.at[cs, zl, ym, x, s2, lanes], sem, recv, "yp")
            put(W.at[cs, zl, yp, x, s3, lanes], sem, recv, "ym")

    def early_ref(g, s):
        c0, c1 = GROUPS[g]
        cs, lanes = pl.ds(c0, c1 - c0), lanes_of(c0 == FULL)
        return W.at[cs, 0, 0, two if s == 0 else pl.ds(0, 1), :, lanes]

    def early_arrived(g, s):
        wait_for(early_ref(g, s), early_sem.at[g, 2 + s])

    def send(c, s):
        def go(group, idx, d):
            put(W.at[(c,) + idx], send_sem.at[group], recv_sem.at[c, s - 2], d)

        if s == 2:
            for d in ("yp", "ym"):
                go(0, (zl, y, al, s0), d)
            for d in ("xp", "xm"):
                go(0, (zl, al, x, s2), d)
            go(0, (zl, y, lo, s1), "zp")
            go(0, (zl, y, hi, s1), "zm")
            go(0, (zl, lo, x, s3), "zp")
            go(0, (zl, hi, x, s3), "zm")
        elif s == 3:
            for d in ("yp", "ym"):
                go(2, (al, y, al, s1), d)
            for d in ("xp", "xm"):
                go(2, (al, al, x, s3), d)
            go(1, (zl, ym, lo, s0), "yp")
            go(1, (zl, yp, hi, s0), "ym")
            go(1, (zl, lo, xm, s2), "xp")
            go(1, (zl, hi, xp, s2), "xm")
        elif s == 4:
            go(3, (zl, lo, al, s0), "zp")
            go(3, (zl, hi, al, s0), "zm")
            go(3, (zl, al, lo, s2), "zp")
            go(3, (zl, al, hi, s2), "zm")
            go(3, (0, ym, al, s1), "yp")
            go(3, (1, yp, al, s1), "ym")
            go(3, (0, al, xm, s3), "xp")
            go(3, (1, al, xp, s3), "xm")

    top, low = pl.ds(0, 32), pl.ds(32, 32)

    def send_late(c, s, half):
        def go(idx, d):
            put(W.at[(c,) + idx + (lanes_of(half),)], send_sem.at[4 + 3 * half + s - 2], recv_sem.at[c, s - 2], d)

        if s == 2:
            go((zl, y, lo, top), "zp")
            go((zl, y, hi, top), "zm")
            go((zl, lo, x, low), "zp")
            go((zl, hi, x, low), "zm")
        elif s == 3:
            for d in ("yp", "ym"):
                go((al, y, al, top), d)
            for d in ("xp", "xm"):
                go((al, al, x, low), d)
        elif s == 4:
            go((0, ym, al, top), "yp")
            go((1, yp, al, top), "ym")
            go((0, al, xm, low), "xp")
            go((1, al, xp, low), "xm")

    def late_refs(cs, half):
        ln = lanes_of(half)
        return [W.at[cs, 0, 0, :, :, ln], W.at[cs, 0, :, :, :, ln], W.at[cs, :, 0, :, :, ln]]

    def arrived(c, s):
        r = [W.at[c, 0, three, two], W.at[pl.ds(0, 5), 0, 0, two], W.at[c, 0, three]][s - 2]
        wait_for(r, recv_sem.at[c, s - 2])

    def drain():
        for g in range(len(GROUPS)):
            for s in range(2):
                wait_for(early_ref(g, s), early_sem.at[g, s])
        cs = pl.ds(0, NORM)
        for i, r in enumerate([W.at[cs, 0, three, two], W.at[cs, 0, 0, two], W.at[cs, :, 0], W.at[cs, 0, three]]):
            wait_for(r, send_sem.at[i])
        for half in range(2):
            for i, r in enumerate(late_refs(pl.ds(FULL, 1) if half else pl.ds(NORM, FULL - NORM), half)):
                wait_for(r, send_sem.at[4 + 3 * half + i])

    def tick(t):
        for s in range(2, 6):
            c = t - LAG * (s - 2)

            @pl.when((c >= 0) & (c < NORM))
            def _():
                if s > 2:
                    arrived(c, s - 1)
                if s < 5:
                    send(c, s)

            def late(half):
                if s > 2:
                    wait_for(late_refs(c, half)[s - 3], recv_sem.at[c, s - 3])
                if s < 5:
                    send_late(c, s, half)

            @pl.when((c >= NORM) & (c < FULL))
            def _():
                late(0)

            @pl.when(c == FULL)
            def _():
                late(1)

    return tick, drain, early, early_arrived


def nt(a, b):
    return lax.dot_general(a, b, (((1,), (1,)), ((), ())), preferred_element_type=F32)


def rows_normed(v, gain):
    return (v * lax.rsqrt(jnp.mean(v * v, axis=-1, keepdims=True) + EPS) * gain).astype(BF16)


def layer(
    w_query, w_key, w_value, w_outt, w_ffgate, w_ffup, w_downt,
    tokens_in, cos_in, sin_in, mix_gain, ffn_gain, tap_gate, tap_up,
    out_hbm,
    W, out, tokens, cos, sin, xn, qs, ks, vs, dec, hidden, mixs, mixr, pre_a, pre_b, act, acc,
    send_sem, recv_sem, early_sem, xsem, lsem, fsem, osem,
):
    where = place()
    zl, y, x, to, partner, tp = where[0], where[1], where[2], where[7], where[8], where[9]
    other = 1 - tp
    tick, drain, early, early_arrived = make_comm(W, send_sem, recv_sem, early_sem, where)

    def load(ref, c, lanes, g):
        pltpu.make_async_copy(ref, W.at[c, zl, y, x, :, lanes], lsem.at[g]).start()

    own_rows = [pltpu.make_async_copy(a, b, lsem.at[k]) for a, b, k in ((tokens_in, tokens, 5), (cos_in, cos, 6), (sin_in, sin, 7))]
    own_rows[0].start()
    left, right, whole = pl.ds(0, 128), pl.ds(128, 128), pl.ds(0, 256)
    for h in range(2):
        load(w_query.at[:, pl.ds(h * 128, 128)], 2 * h, left, h)
        load(w_key.at[:, pl.ds(h * 128, 128)], 2 * h, right, h)
        load(w_value.at[:, pl.ds(h * 256, 256)], 2 * h + 1, whole, h)
    for i in range(2):
        load(w_outt.at[:, pl.ds(i * 256, 256)], OUT_C + i, whole, 1)
    for j in range(FFC):
        g = 2 if GU_C + j < GROUPS[2][1] else 3
        load(w_ffgate.at[:, pl.ds(j * 128, 128)], GU_C + j, left, g)
        load(w_ffup.at[:, pl.ds(j * 128, 128)], GU_C + j, right, g)
    for i in range(5):
        load(w_downt.at[:, pl.ds(i * 256, 256)], DOWN_C + i, whole, 3)
    load(w_downt.at[:, pl.ds(1280, 128)], FULL, left, 4)
    own_rows[1].start()
    own_rows[2].start()

    def loaded(g):
        c0, c1 = GROUPS[g]
        wait_for(W.at[pl.ds(c0, c1 - c0), zl, y, x, :, left if g == 4 else whole], lsem.at[g])

    barrier = pltpu.get_barrier_semaphore()
    for d in list(to.values()) + [partner]:
        pl.semaphore_signal(barrier, inc=1, device_id=d, device_id_type=MESH)
    pl.semaphore_wait(barrier, 7)

    def hand(src_ref, dst_ref, k):
        pltpu.make_async_remote_copy(
            src_ref=src_ref, dst_ref=dst_ref, send_sem=xsem.at[k], recv_sem=xsem.at[k + 1],
            device_id=partner, device_id_type=MESH,
        ).start()

    def rows_of(i):
        return pl.ds(pl.multiple_of(i * 128, 128), 128)

    def cols_of(n):
        return pl.ds(pl.multiple_of(n * 256, 256), 256)

    def hand_rows(i, k):
        r = xn.at[tp, rows_of(i)]
        hand(r, r, k)

    def norm_own(i):
        def one(k, _):
            r = pl.ds(pl.multiple_of(i * 128 + k * 32, 32), 32)
            xn[tp, r, :] = rows_normed(tokens[r, :].astype(F32), mix_gain[...])
            return 0

        lax.fori_loop(0, 4, one, 0)

    def tables():
        place_i = lax.broadcasted_iota(jnp.int32, (128, 128), 0).astype(F32)
        place_m = lax.broadcasted_iota(jnp.int32, (128, 128), 1).astype(F32)
        for h in range(2):
            g = jnp.full((128, 128), (tp * 2 + h).astype(F32))
            rate = (1.0 / 16.0) * jnp.exp(g * (np.log(32.0 / LENGTH) / (HEADS - 1)).astype(np.float32))
            gap = place_i - place_m
            dec[h, 0] = jnp.where(gap >= 0, jnp.exp(-jnp.maximum(gap, 0.0) * rate), 0.0)
            dec[h, 1] = jnp.exp(-(127.0 - place_i) * rate)
            dec[h, 2] = jnp.exp(-(place_i + 1.0) * rate)
            dec[h, 3] = jnp.exp(-128.0 * rate)
        pre_a[0:8, :] = jnp.zeros((8, 256), F32)

        def clear(i, _):
            pre_b[pl.ds(pl.multiple_of(i * 8, 8), 8), :] = jnp.zeros((8, 256), F32)
            return 0

        lax.fori_loop(0, (8 + LENGTH) // 8, clear, 0)

    def project(c, half):
        return jnp.dot(xn[half], W[c].reshape(2048, 256), preferred_element_type=F32)

    def qk_step(h):
        def one(half, _):
            u = project(2 * h, half).astype(BF16).astype(F32)
            r = pl.ds(pl.multiple_of(half * HALF, HALF), HALF)
            cs, sn = cos[r, :], sin[r, :]
            q, k = u[:, :128], u[:, 128:]
            qs[r, :] = (q * cs + pltpu.roll(q, 64, 1) * sn).astype(BF16)
            ks[r, :] = ((k * cs + pltpu.roll(k, 64, 1) * sn) * DK ** (-0.5)).astype(BF16)
            return 0

        lax.fori_loop(0, 2, one, 0)

    def v_step(h):
        def one(half, _):
            vs[pl.ds(pl.multiple_of(half * HALF, HALF), HALF), :] = project(2 * h + 1, half).astype(BF16)
            return 0

        lax.fori_loop(0, 2, one, 0)

    def retain(h):
        onset = jnp.concatenate([dec[h, 2]] * 2, axis=1)
        passing = jnp.concatenate([dec[h, 3]] * 2, axis=1)
        state = jnp.zeros((128, 256), F32)
        for b in range(8):
            r = slice(b * 128, b * 128 + 128)
            q, k, v = qs[r, :], ks[r, :], vs[r, :]
            weights = (nt(q, k) * dec[h, 0]).astype(BF16)
            ret = jnp.dot(weights, v, preferred_element_type=F32)
            if b:
                ret = ret + jnp.dot(q, state.astype(BF16), preferred_element_type=F32) * onset
            if b < 7:
                kd = (k.astype(F32) * dec[h, 1]).astype(BF16)
                fresh = lax.dot_general(kd, v, (((0,), (0,)), ((), ())), preferred_element_type=F32)
                state = state * passing + fresh if b else fresh
            cen = ret - jnp.mean(ret, axis=-1, keepdims=True)
            hidden[h, r, :] = (cen * lax.rsqrt(jnp.mean(cen * cen, axis=-1, keepdims=True) + EPS)).astype(BF16)

    def tile(c, n):
        return W[c, n // 4, n % 4].reshape(256, 256)

    def out_rows(half, n):
        r = pl.ds(pl.multiple_of(half * HALF, HALF), HALF)
        return nt(hidden[0, r, :], tile(OUT_C, n)) + nt(hidden[1, r, :], tile(OUT_C + 1, n))

    def send_cols(n, k):
        hand(mixs.at[:, cols_of(n)], mixr.at[:, cols_of(n)], k)

    def out_partner():
        def one(n, _):
            mixs[:, cols_of(n)] = out_rows(other, n).astype(BF16)

            @pl.when(n > 0)
            def _():
                send_cols(n - 1, 2)

            return 0

        lax.fori_loop(0, 8, one, 0)

    def out_own():
        def one(n, _):
            acc[0, :, cols_of(n)] = out_rows(tp, n).astype(BF16).astype(F32)

            @pl.when(n == 0)
            def _():
                send_cols(7, 2)

            return 0

        lax.fori_loop(0, 8, one, 0)

    def middle():
        wait_for(xn.at[0], xsem.at[0])
        wait_for(mixr, xsem.at[3])

        def one(i, _):
            for k in range(4):
                r = pl.ds(pl.multiple_of(i * 128 + k * 32, 32), 32)
                resid = (tokens[r, :].astype(F32) + (acc[0, r, :] + mixr[r, :].astype(F32))).astype(BF16)
                out[r, :] = resid
                xn[tp, r, :] = rows_normed(resid.astype(F32), ffn_gain[...])

            @pl.when(i > 0)
            def _():
                hand_rows(i - 1, 4)

            return 0

        lax.fori_loop(0, 4, one, 0)

    def gu_dot(j, half, pre):
        r = pl.ds(pl.multiple_of(8 + half * HALF, 8), HALF)
        pre[r, :] = project(GU_C + j, half).astype(BF16).astype(F32)

    def gu_conv(j, half, pre):
        mine = pl.ds(pl.multiple_of(tp * (FFC * 128) + j * 128, 128), 128)
        k0, k1, k2 = (
            jnp.concatenate([tap_gate[k : k + 1, mine], tap_up[k : k + 1, mine]], axis=1) for k in range(3)
        )
        lane = pl.ds(pl.multiple_of((j % 2) * 128, 128), 128)
        for i in range(8):
            u = pre[pl.ds(pl.multiple_of(half * HALF + i * 64, 64), 72), :]
            conv = k0 * pltpu.roll(u, 2, 0) + k1 * pltpu.roll(u, 1, 0) + k2 * u
            g, w = conv[8:, :128], conv[8:, 128:]
            act[j // 2, half, i * 64 : i * 64 + 64, lane] = (g / (1.0 + jnp.exp(-g)) * w).astype(BF16)

    def gu_step(j, now, before):
        last = jnp.maximum(j - 1, 0)
        gu_dot(j, tp, now)
        gu_conv(last, tp, before)

        @pl.when(j == 0)
        def _():
            hand_rows(3, 4)
            wait_for(xn.at[0], xsem.at[5])

        gu_dot(j, other, now)
        gu_conv(last, other, before)

    def down_part(first, count):
        def one(i, _):
            for k in range(2):
                n = 2 * i + k
                for half in range(2):
                    o = nt(act[first, half], tile(DOWN_C + first, n))
                    for d in range(1, count):
                        o = o + nt(act[first + d, half], tile(DOWN_C + first + d, n))
                    acc[half, :, cols_of(n)] = acc[half, :, cols_of(n)] + o if first else o
            return 0

        lax.fori_loop(0, 4, one, 0)

    def down_rows(half, n):
        o = acc[half, :, cols_of(n)] + nt(act[5, half, :, :128], tile(DOWN_C + 5, n)[:, :128])
        return o.astype(BF16)

    def send_piece(n):
        pltpu.make_async_remote_copy(
            src_ref=mixs.at[:, cols_of(n)], dst_ref=mixr.at[:, cols_of(n)], send_sem=xsem.at[6], recv_sem=fsem.at[n],
            device_id=partner, device_id_type=MESH,
        ).start()

    def put_out(i):
        c = pl.ds(pl.multiple_of(i * 512, 512), 512)
        return pltpu.make_async_copy(out.at[:, c], out_hbm.at[:, c], osem)

    def down_last():
        wait_for(mixs, xsem.at[2])

        def one(i, _):
            for k in range(2):
                mixs[:, cols_of(2 * i + k)] = down_rows(other, 2 * i + k)

            @pl.when(i > 0)
            def _():
                send_piece(2 * i - 2)
                send_piece(2 * i - 1)

            return 0

        lax.fori_loop(0, 4, one, 0)

        def two(i, _):
            mine = [down_rows(tp, 2 * i + k).astype(F32) for k in range(2)]

            @pl.when(i == 0)
            def _():
                send_piece(6)
                send_piece(7)

            for k in range(2):
                n = 2 * i + k
                wait_for(mixr.at[:, pl.ds(0, 256)], fsem.at[n])
                out[:, cols_of(n)] = (
                    out[:, cols_of(n)].astype(F32) + (mine[k] + mixr[:, cols_of(n)].astype(F32))
                ).astype(BF16)

            @pl.when(i > 0)
            def _():
                put_out(i - 1).start()

            return 0

        lax.fori_loop(0, 4, two, 0)
        put_out(3).start()
        wait_for(xn.at[0], xsem.at[4])
        wait_for(mixs, xsem.at[6])

    GU0 = READY + GU_C + 2
    NORM0 = READY - 5
    LAST = READY + C - 1

    loaded(0)
    early(0, 0)
    loaded(1)
    early(1, 0)
    early_arrived(0, 0)
    early(0, 1)
    loaded(2)
    early(2, 0)
    early_arrived(1, 0)
    early(1, 1)

    def step(t, _):
        for g in (0, 1, 2, 3, 4):
            @pl.when(t == GROUPS[g][0])
            def _():
                early_arrived(g, 1)

        tick(t)

        @pl.when(t == 1)
        def _():
            for g in (3, 4):
                loaded(g)
                early(g, 0)

        @pl.when(t == 2)
        def _():
            early_arrived(2, 0)
            early(2, 1)

        @pl.when(t == 4)
        def _():
            for g in (3, 4):
                early_arrived(g, 0)
                early(g, 1)

        @pl.when(t == NORM0)
        def _():
            own_rows[0].wait()

        @pl.when((t >= NORM0) & (t < NORM0 + 4))
        def _():
            norm_own(t - NORM0)

        @pl.when((t > NORM0) & (t <= NORM0 + 4))
        def _():
            hand_rows(t - NORM0 - 1, 0)

        @pl.when(t == NORM0 - 1)
        def _():
            tables()

        @pl.when(t == READY)
        def _():
            own_rows[1].wait()
            own_rows[2].wait()
            wait_for(xn.at[0], xsem.at[1])

        @pl.when((t == READY) | (t == READY + 2))
        def _():
            qk_step((t - READY) // 2)

        @pl.when((t == READY + 1) | (t == READY + 3))
        def _():
            v_step((t - READY - 1) // 2)

        @pl.when((t == READY + 1) | (t == READY + 4))
        def _():
            retain((t - READY - 1) // 3)

        @pl.when(t == READY + 5)
        def _():
            out_partner()

        @pl.when(t == READY + 6)
        def _():
            out_own()

        @pl.when(t == READY + 7)
        def _():
            middle()

        @pl.when((t >= GU0) & (t < GU0 + FFC) & ((t - GU0) % 2 == 0))
        def _():
            gu_step(t - GU0, pre_a, pre_b)

        @pl.when((t >= GU0) & (t < GU0 + FFC) & ((t - GU0) % 2 == 1))
        def _():
            gu_step(t - GU0, pre_b, pre_a)

        @pl.when(t == GU0 + FFC)
        def _():
            lax.fori_loop(0, 2, lambda half, _: (gu_conv(FFC - 1, half, pre_a), 0)[1], 0)

        @pl.when(t == LAST - 3)
        def _():
            down_part(0, 3)

        @pl.when(t == LAST - 1)
        def _():
            down_part(3, 2)

        @pl.when(t == LAST)
        def _():
            down_last()

        return 0

    lax.fori_loop(0, LAST + 1, step, 0)
    wait_for(out, osem)
    drain()


def deliver(a, b, held, sems):
    pieces = [pl.ds(i * 128, 128) for i in range(4)]
    for i, r in enumerate(pieces):
        pltpu.make_async_copy(a.at[r], held.at[r], sems.at[i]).start()
    for i, r in enumerate(pieces):
        pltpu.make_async_copy(a.at[r], held.at[r], sems.at[i]).wait()
        pltpu.make_async_copy(held.at[r], b.at[r], sems.at[4 + i]).start()
    for i, r in enumerate(pieces):
        pltpu.make_async_copy(held.at[r], b.at[r], sems.at[4 + i]).wait()


def angle_tables():
    inverse = 10000.0 ** (-np.arange(64) * 2.0 / 128)
    angles = np.arange(LENGTH)[:, None] * inverse[None, :]
    cos, sin = np.cos(angles), np.sin(angles)
    return (
        np.concatenate([cos, cos], axis=1).astype(np.float32),
        np.concatenate([-sin, sin], axis=1).astype(np.float32),
    )


def body(
    tokens, mix_gain, w_query, w_key, w_value, w_out, ffn_gain, w_ffgate, w_ffup, conv_gate, conv_up, w_down
):
    cos, sin = angle_tables()
    vmem = pl.BlockSpec(memory_space=pltpu.VMEM)
    hbm = pl.BlockSpec(memory_space=pl.ANY)
    whole = jax.ShapeDtypeStruct((HALF, D), BF16)
    done = pl.pallas_call(
        layer,
        out_shape=whole,
        in_specs=[hbm] * 10 + [vmem] * 4,
        out_specs=hbm,
        scratch_shapes=[
            pltpu.VMEM((C, 2, 4, 4, 64, COLS), BF16),
            pltpu.VMEM((HALF, D), BF16),
            pltpu.VMEM((HALF, D), BF16),
            pltpu.VMEM((LENGTH, 128), F32),
            pltpu.VMEM((LENGTH, 128), F32),
            pltpu.VMEM((2, HALF, D), BF16),
            pltpu.VMEM((LENGTH, 128), BF16),
            pltpu.VMEM((LENGTH, 128), BF16),
            pltpu.VMEM((LENGTH, 256), BF16),
            pltpu.VMEM((2, 4, 128, 128), F32),
            pltpu.VMEM((2, LENGTH, 256), BF16),
            pltpu.VMEM((HALF, D), BF16),
            pltpu.VMEM((HALF, D), BF16),
            pltpu.VMEM((8 + LENGTH, 256), F32),
            pltpu.VMEM((8 + LENGTH, 256), F32),
            pltpu.VMEM((6, 2, HALF, 256), BF16),
            pltpu.VMEM((2, HALF, D), F32),
            pltpu.SemaphoreType.DMA((10,)),
            pltpu.SemaphoreType.DMA((C, 3)),
            pltpu.SemaphoreType.DMA((len(GROUPS), 4)),
            pltpu.SemaphoreType.DMA((8,)),
            pltpu.SemaphoreType.DMA((8,)),
            pltpu.SemaphoreType.DMA((8,)),
            pltpu.SemaphoreType.DMA,
        ],
        compiler_params=pltpu.CompilerParams(
            collective_id=0, has_side_effects=True, vmem_limit_bytes=VLIM
        ),
    )(
        w_query, w_key, w_value, w_out.T, w_ffgate, w_ffup, w_down.T,
        tokens, jnp.asarray(cos), jnp.asarray(sin), mix_gain.reshape(1, D), ffn_gain.reshape(1, D), conv_gate, conv_up,
    )
    return pl.pallas_call(
        deliver,
        out_shape=whole,
        in_specs=[hbm],
        out_specs=hbm,
        scratch_shapes=[pltpu.VMEM((HALF, D), BF16), pltpu.SemaphoreType.DMA((8,))],
        compiler_params=pltpu.CompilerParams(vmem_limit_bytes=67043328),
    )(done)


def solution(mesh):
    w = P("fs", "tp")
    placed = (P(("rep", "fs", "tp"), None), P(), w, w, w, P("tp", "fs"), P(), w, w, P(), P(), P("tp", "fs"))
    return jax.shard_map(
        body, mesh=mesh, in_specs=placed, out_specs=P(("rep", "fs", "tp"), None), check_vma=False
    )
```

```python
import jax
import jax.numpy as jnp
import numpy as np
from jax import lax
from jax.experimental import pallas as pl
from jax.experimental.pallas import tpu as pltpu
from jax.sharding import PartitionSpec as P

MESH = pl.DeviceIdType.MESH
HEADS = 4
DK = 128
D = 2048
BLOCK = 128
LENGTH = 1024
HALF = 512
EPS = 1e-6
C = 23
COLS = 256
LAG = 3
READY = 3 * LAG
FULL = 22
VLIM = 67043328
NORM = 20
GROUPS = ((0, 2), (2, 6), (6, 14), (14, 22), (22, 23))
OUT_C = 4
GU_C = 6
DOWN_C = 17
FFC = 11
F32 = jnp.float32
BF16 = jnp.bfloat16


def place():
    rep = lax.axis_index("rep")
    fs = lax.axis_index("fs")
    tp = lax.axis_index("tp")
    zl, y, x = fs // 16, (fs // 4) % 4, fs % 4
    z = rep * 2 + zl

    def dev(z_, y_, x_):
        return (z_ // 2, (z_ % 2) * 16 + y_ * 4 + x_, tp)

    xp, xm, yp, ym = (x + 1) % 4, (x + 3) % 4, (y + 1) % 4, (y + 3) % 4
    zp, zm = (z + 1) % 4, (z + 3) % 4
    to = dict(
        xp=dev(z, y, xp), xm=dev(z, y, xm), yp=dev(z, yp, x), ym=dev(z, ym, x), zp=dev(zp, y, x), zm=dev(zm, y, x)
    )
    return zl, y, x, xp, xm, yp, ym, to, (rep, fs, 1 - tp), tp


def wait_for(ref, sem):
    pltpu.make_async_copy(ref, ref, sem).wait()


def make_comm(W, send_sem, recv_sem, early_sem, where):
    zl, y, x, xp, xm, yp, ym, to, partner, tp = where
    s0, s1, s2, s3 = (pl.ds(16 * i, 16) for i in range(4))
    lo, hi, al = pl.ds(0, 2), pl.ds(2, 2), slice(None)
    two, three = pl.ds(0, 2), pl.ds(0, 3)

    def put(r, sem, recv, d):
        pltpu.make_async_remote_copy(
            src_ref=r, dst_ref=r, send_sem=sem, recv_sem=recv, device_id=to[d], device_id_type=MESH
        ).start()

    def lanes_of(half):
        return pl.ds(0, 128) if half else pl.ds(0, 256)

    def early(g, s):
        c0, c1 = GROUPS[g]
        cs, lanes = pl.ds(c0, c1 - c0), lanes_of(c0 == FULL)
        sem, recv = early_sem.at[g, s], early_sem.at[g, 2 + s]
        if s == 0:
            for d in ("xp", "xm"):
                put(W.at[cs, zl, y, x, pl.ds(0, 32), lanes], sem, recv, d)
            for d in ("yp", "ym"):
                put(W.at[cs, zl, y, x, pl.ds(32, 32), lanes], sem, recv, d)
        else:
            put(W.at[cs, zl, y, xm, s0, lanes], sem, recv, "xp")
            put(W.at[cs, zl, y, xp, s1, lanes], sem, recv, "xm")
            put(W.at[cs, zl, ym, x, s2, lanes], sem, recv, "yp")
            put(W.at[cs, zl, yp, x, s3, lanes], sem, recv, "ym")

    def early_ref(g, s):
        c0, c1 = GROUPS[g]
        cs, lanes = pl.ds(c0, c1 - c0), lanes_of(c0 == FULL)
        return W.at[cs, 0, 0, two if s == 0 else pl.ds(0, 1), :, lanes]

    def early_arrived(g, s):
        wait_for(early_ref(g, s), early_sem.at[g, 2 + s])

    def send(c, s):
        def go(group, idx, d):
            put(W.at[(c,) + idx], send_sem.at[group], recv_sem.at[c, s - 2], d)

        if s == 2:
            for d in ("yp", "ym"):
                go(0, (zl, y, al, s0), d)
            for d in ("xp", "xm"):
                go(0, (zl, al, x, s2), d)
            go(0, (zl, y, lo, s1), "zp")
            go(0, (zl, y, hi, s1), "zm")
            go(0, (zl, lo, x, s3), "zp")
            go(0, (zl, hi, x, s3), "zm")
        elif s == 3:
            for d in ("yp", "ym"):
                go(2, (al, y, al, s1), d)
            for d in ("xp", "xm"):
                go(2, (al, al, x, s3), d)
            go(1, (zl, ym, lo, s0), "yp")
            go(1, (zl, yp, hi, s0), "ym")
            go(1, (zl, lo, xm, s2), "xp")
            go(1, (zl, hi, xp, s2), "xm")
        elif s == 4:
            go(3, (zl, lo, al, s0), "zp")
            go(3, (zl, hi, al, s0), "zm")
            go(3, (zl, al, lo, s2), "zp")
            go(3, (zl, al, hi, s2), "zm")
            go(3, (0, ym, al, s1), "yp")
            go(3, (1, yp, al, s1), "ym")
            go(3, (0, al, xm, s3), "xp")
            go(3, (1, al, xp, s3), "xm")

    top, low = pl.ds(0, 32), pl.ds(32, 32)

    def send_late(c, s, half):
        def go(idx, d):
            put(W.at[(c,) + idx + (lanes_of(half),)], send_sem.at[4 + 3 * half + s - 2], recv_sem.at[c, s - 2], d)

        if s == 2:
            go((zl, y, lo, top), "zp")
            go((zl, y, hi, top), "zm")
            go((zl, lo, x, low), "zp")
            go((zl, hi, x, low), "zm")
        elif s == 3:
            for d in ("yp", "ym"):
                go((al, y, al, top), d)
            for d in ("xp", "xm"):
                go((al, al, x, low), d)
        elif s == 4:
            go((0, ym, al, top), "yp")
            go((1, yp, al, top), "ym")
            go((0, al, xm, low), "xp")
            go((1, al, xp, low), "xm")

    def late_refs(cs, half):
        ln = lanes_of(half)
        return [W.at[cs, 0, 0, :, :, ln], W.at[cs, 0, :, :, :, ln], W.at[cs, :, 0, :, :, ln]]

    def arrived(c, s):
        r = [W.at[c, 0, three, two], W.at[pl.ds(0, 5), 0, 0, two], W.at[c, 0, three]][s - 2]
        wait_for(r, recv_sem.at[c, s - 2])

    def drain():
        for g in range(len(GROUPS)):
            for s in range(2):
                wait_for(early_ref(g, s), early_sem.at[g, s])
        cs = pl.ds(0, NORM)
        for i, r in enumerate([W.at[cs, 0, three, two], W.at[cs, 0, 0, two], W.at[cs, :, 0], W.at[cs, 0, three]]):
            wait_for(r, send_sem.at[i])
        for half in range(2):
            for i, r in enumerate(late_refs(pl.ds(FULL, 1) if half else pl.ds(NORM, FULL - NORM), half)):
                wait_for(r, send_sem.at[4 + 3 * half + i])

    def tick(t):
        for s in (5, 4, 3, 2):
            c = t - LAG * (s - 2)

            @pl.when((c >= 0) & (c < NORM))
            def _():
                if s > 2:
                    arrived(c, s - 1)
                if s < 5:
                    send(c, s)

            def late(half):
                if s > 2:
                    wait_for(late_refs(c, half)[s - 3], recv_sem.at[c, s - 3])
                if s < 5:
                    send_late(c, s, half)

            @pl.when((c >= NORM) & (c < FULL))
            def _():
                late(0)

            @pl.when(c == FULL)
            def _():
                late(1)

    return tick, drain, early, early_arrived


def nt(a, b):
    return lax.dot_general(a, b, (((1,), (1,)), ((), ())), preferred_element_type=F32)


def rows_normed(v, gain):
    return (v * lax.rsqrt(jnp.mean(v * v, axis=-1, keepdims=True) + EPS) * gain).astype(BF16)


def layer(
    w_query, w_key, w_value, w_outt, w_ffgate, w_ffup, w_downt,
    tokens_in, cos_in, sin_in, mix_gain, ffn_gain, tap_gate, tap_up,
    out_hbm,
    W, out, tokens, cos, sin, xn, qs, ks, vs, dec, hidden, mixs, mixr, pre_a, pre_b, act, acc,
    send_sem, recv_sem, early_sem, xsem, lsem, fsem, osem,
):
    where = place()
    zl, y, x, to, partner, tp = where[0], where[1], where[2], where[7], where[8], where[9]
    other = 1 - tp
    tick, drain, early, early_arrived = make_comm(W, send_sem, recv_sem, early_sem, where)

    def load(ref, c, lanes, g):
        pltpu.make_async_copy(ref, W.at[c, zl, y, x, :, lanes], lsem.at[g]).start()

    own_rows = [pltpu.make_async_copy(a, b, lsem.at[k]) for a, b, k in ((tokens_in, tokens, 5), (cos_in, cos, 6), (sin_in, sin, 7))]
    own_rows[0].start()
    left, right, whole = pl.ds(0, 128), pl.ds(128, 128), pl.ds(0, 256)
    for h in range(2):
        load(w_query.at[:, pl.ds(h * 128, 128)], 2 * h, left, h)
        load(w_key.at[:, pl.ds(h * 128, 128)], 2 * h, right, h)
        load(w_value.at[:, pl.ds(h * 256, 256)], 2 * h + 1, whole, h)
    for i in range(2):
        load(w_outt.at[:, pl.ds(i * 256, 256)], OUT_C + i, whole, 1)
    for j in range(FFC):
        g = 2 if GU_C + j < GROUPS[2][1] else 3
        load(w_ffgate.at[:, pl.ds(j * 128, 128)], GU_C + j, left, g)
        load(w_ffup.at[:, pl.ds(j * 128, 128)], GU_C + j, right, g)
    for i in range(5):
        load(w_downt.at[:, pl.ds(i * 256, 256)], DOWN_C + i, whole, 3)
    load(w_downt.at[:, pl.ds(1280, 128)], FULL, left, 4)
    own_rows[1].start()
    own_rows[2].start()

    def loaded(g):
        c0, c1 = GROUPS[g]
        wait_for(W.at[pl.ds(c0, c1 - c0), zl, y, x, :, left if g == 4 else whole], lsem.at[g])

    barrier = pltpu.get_barrier_semaphore()
    for d in list(to.values()) + [partner]:
        pl.semaphore_signal(barrier, inc=1, device_id=d, device_id_type=MESH)
    pl.semaphore_wait(barrier, 7)

    def hand(src_ref, dst_ref, k):
        pltpu.make_async_remote_copy(
            src_ref=src_ref, dst_ref=dst_ref, send_sem=xsem.at[k], recv_sem=xsem.at[k + 1],
            device_id=partner, device_id_type=MESH,
        ).start()

    def rows_of(i):
        return pl.ds(pl.multiple_of(i * 128, 128), 128)

    def cols_of(n):
        return pl.ds(pl.multiple_of(n * 256, 256), 256)

    def hand_rows(i, k):
        r = xn.at[tp, rows_of(i)]
        hand(r, r, k)

    def norm_own(i):
        def one(k, _):
            r = pl.ds(pl.multiple_of(i * 128 + k * 32, 32), 32)
            xn[tp, r, :] = rows_normed(tokens[r, :].astype(F32), mix_gain[...])
            return 0

        lax.fori_loop(0, 4, one, 0)

    def tables():
        place_i = lax.broadcasted_iota(jnp.int32, (128, 128), 0).astype(F32)
        place_m = lax.broadcasted_iota(jnp.int32, (128, 128), 1).astype(F32)
        for h in range(2):
            g = jnp.full((128, 128), (tp * 2 + h).astype(F32))
            rate = (1.0 / 16.0) * jnp.exp(g * (np.log(32.0 / LENGTH) / (HEADS - 1)).astype(np.float32))
            gap = place_i - place_m
            dec[h, 0] = jnp.where(gap >= 0, jnp.exp(-jnp.maximum(gap, 0.0) * rate), 0.0)
            dec[h, 1] = jnp.exp(-(127.0 - place_i) * rate)
            dec[h, 2] = jnp.exp(-(place_i + 1.0) * rate)
            dec[h, 3] = jnp.exp(-128.0 * rate)
        pre_a[0:8, :] = jnp.zeros((8, 256), F32)

        def clear(i, _):
            pre_b[pl.ds(pl.multiple_of(i * 8, 8), 8), :] = jnp.zeros((8, 256), F32)
            return 0

        lax.fori_loop(0, (8 + LENGTH) // 8, clear, 0)

    def project(c, half):
        return jnp.dot(xn[half], W[c].reshape(2048, 256), preferred_element_type=F32)

    def qk_step(h):
        def one(half, _):
            u = project(2 * h, half).astype(BF16).astype(F32)
            r = pl.ds(pl.multiple_of(half * HALF, HALF), HALF)
            cs, sn = cos[r, :], sin[r, :]
            q, k = u[:, :128], u[:, 128:]
            qs[r, :] = (q * cs + pltpu.roll(q, 64, 1) * sn).astype(BF16)
            ks[r, :] = ((k * cs + pltpu.roll(k, 64, 1) * sn) * DK ** (-0.5)).astype(BF16)
            return 0

        lax.fori_loop(0, 2, one, 0)

    def v_step(h):
        def one(half, _):
            vs[pl.ds(pl.multiple_of(half * HALF, HALF), HALF), :] = project(2 * h + 1, half).astype(BF16)
            return 0

        lax.fori_loop(0, 2, one, 0)

    def retain(h):
        onset = jnp.concatenate([dec[h, 2]] * 2, axis=1)
        passing = jnp.concatenate([dec[h, 3]] * 2, axis=1)
        state = jnp.zeros((128, 256), F32)
        for b in range(8):
            r = slice(b * 128, b * 128 + 128)
            q, k, v = qs[r, :], ks[r, :], vs[r, :]
            weights = (nt(q, k) * dec[h, 0]).astype(BF16)
            ret = jnp.dot(weights, v, preferred_element_type=F32)
            if b:
                ret = ret + jnp.dot(q, state.astype(BF16), preferred_element_type=F32) * onset
            if b < 7:
                kd = (k.astype(F32) * dec[h, 1]).astype(BF16)
                fresh = lax.dot_general(kd, v, (((0,), (0,)), ((), ())), preferred_element_type=F32)
                state = state * passing + fresh if b else fresh
            cen = ret - jnp.mean(ret, axis=-1, keepdims=True)
            hidden[h, r, :] = (cen * lax.rsqrt(jnp.mean(cen * cen, axis=-1, keepdims=True) + EPS)).astype(BF16)

    def tile(c, n):
        return W[c, n // 4, n % 4].reshape(256, 256)

    def out_rows(half, n):
        r = pl.ds(pl.multiple_of(half * HALF, HALF), HALF)
        return nt(hidden[0, r, :], tile(OUT_C, n)) + nt(hidden[1, r, :], tile(OUT_C + 1, n))

    def send_cols(n, k):
        hand(mixs.at[:, cols_of(n)], mixr.at[:, cols_of(n)], k)

    def out_partner():
        def one(n, _):
            mixs[:, cols_of(n)] = out_rows(other, n).astype(BF16)

            @pl.when(n > 0)
            def _():
                send_cols(n - 1, 2)

            return 0

        lax.fori_loop(0, 8, one, 0)

    def out_own():
        def one(n, _):
            acc[0, :, cols_of(n)] = out_rows(tp, n).astype(BF16).astype(F32)

            @pl.when(n == 0)
            def _():
                send_cols(7, 2)

            return 0

        lax.fori_loop(0, 8, one, 0)

    def middle():
        wait_for(xn.at[0], xsem.at[0])
        wait_for(mixr, xsem.at[3])

        def one(i, _):
            for k in range(4):
                r = pl.ds(pl.multiple_of(i * 128 + k * 32, 32), 32)
                resid = (tokens[r, :].astype(F32) + (acc[0, r, :] + mixr[r, :].astype(F32))).astype(BF16)
                out[r, :] = resid
                xn[tp, r, :] = rows_normed(resid.astype(F32), ffn_gain[...])

            @pl.when(i > 0)
            def _():
                hand_rows(i - 1, 4)

            return 0

        lax.fori_loop(0, 4, one, 0)

    def gu_dot(j, half, pre):
        r = pl.ds(pl.multiple_of(8 + half * HALF, 8), HALF)
        pre[r, :] = project(GU_C + j, half).astype(BF16).astype(F32)

    def gu_conv(j, half, pre):
        mine = pl.ds(pl.multiple_of(tp * (FFC * 128) + j * 128, 128), 128)
        k0, k1, k2 = (
            jnp.concatenate([tap_gate[k : k + 1, mine], tap_up[k : k + 1, mine]], axis=1) for k in range(3)
        )
        lane = pl.ds(pl.multiple_of((j % 2) * 128, 128), 128)
        for i in range(8):
            u = pre[pl.ds(pl.multiple_of(half * HALF + i * 64, 64), 72), :]
            conv = k0 * pltpu.roll(u, 2, 0) + k1 * pltpu.roll(u, 1, 0) + k2 * u
            g, w = conv[8:, :128], conv[8:, 128:]
            act[j // 2, half, i * 64 : i * 64 + 64, lane] = (g / (1.0 + jnp.exp(-g)) * w).astype(BF16)

    def gu_step(j, now, before):
        last = jnp.maximum(j - 1, 0)
        gu_dot(j, tp, now)
        gu_conv(last, tp, before)

        @pl.when(j == 0)
        def _():
            hand_rows(3, 4)
            wait_for(xn.at[0], xsem.at[5])

        gu_dot(j, other, now)
        gu_conv(last, other, before)

    def down_part(first, count):
        def one(i, _):
            for k in range(2):
                n = 2 * i + k
                for half in range(2):
                    o = nt(act[first, half], tile(DOWN_C + first, n))
                    for d in range(1, count):
                        o = o + nt(act[first + d, half], tile(DOWN_C + first + d, n))
                    acc[half, :, cols_of(n)] = acc[half, :, cols_of(n)] + o if first else o
            return 0

        lax.fori_loop(0, 4, one, 0)

    def down_rows(half, n):
        o = acc[half, :, cols_of(n)] + nt(act[5, half, :, :128], tile(DOWN_C + 5, n)[:, :128])
        return o.astype(BF16)

    def send_piece(n):
        pltpu.make_async_remote_copy(
            src_ref=mixs.at[:, cols_of(n)], dst_ref=mixr.at[:, cols_of(n)], send_sem=xsem.at[6], recv_sem=fsem.at[n],
            device_id=partner, device_id_type=MESH,
        ).start()

    def put_out(i):
        c = pl.ds(pl.multiple_of(i * 512, 512), 512)
        return pltpu.make_async_copy(out.at[:, c], out_hbm.at[:, c], osem)

    def down_last():
        wait_for(mixs, xsem.at[2])

        def one(i, _):
            for k in range(2):
                mixs[:, cols_of(2 * i + k)] = down_rows(other, 2 * i + k)

            @pl.when(i > 0)
            def _():
                send_piece(2 * i - 2)
                send_piece(2 * i - 1)

            return 0

        lax.fori_loop(0, 4, one, 0)

        def two(i, _):
            mine = [down_rows(tp, 2 * i + k).astype(F32) for k in range(2)]

            @pl.when(i == 0)
            def _():
                send_piece(6)
                send_piece(7)

            for k in range(2):
                n = 2 * i + k
                wait_for(mixr.at[:, pl.ds(0, 256)], fsem.at[n])
                out[:, cols_of(n)] = (
                    out[:, cols_of(n)].astype(F32) + (mine[k] + mixr[:, cols_of(n)].astype(F32))
                ).astype(BF16)

            @pl.when(i > 0)
            def _():
                put_out(i - 1).start()

            return 0

        lax.fori_loop(0, 4, two, 0)
        put_out(3).start()
        wait_for(xn.at[0], xsem.at[4])
        wait_for(mixs, xsem.at[6])

    GU0 = READY + GU_C + 2
    NORM0 = READY - 5
    LAST = READY + C - 1

    loaded(0)
    early(0, 0)
    loaded(1)
    early(1, 0)
    early_arrived(0, 0)
    early(0, 1)
    loaded(2)
    early(2, 0)
    early_arrived(1, 0)
    early(1, 1)

    def step(t, _):
        for g in (0, 1, 2, 3, 4):
            @pl.when(t == GROUPS[g][0])
            def _():
                early_arrived(g, 1)

        tick(t)

        @pl.when(t == 1)
        def _():
            for g in (3, 4):
                loaded(g)
                early(g, 0)

        @pl.when(t == 2)
        def _():
            early_arrived(2, 0)
            early(2, 1)

        @pl.when(t == 4)
        def _():
            for g in (3, 4):
                early_arrived(g, 0)
                early(g, 1)

        @pl.when(t == NORM0)
        def _():
            own_rows[0].wait()

        @pl.when((t >= NORM0) & (t < NORM0 + 4))
        def _():
            norm_own(t - NORM0)

        @pl.when((t > NORM0) & (t <= NORM0 + 4))
        def _():
            hand_rows(t - NORM0 - 1, 0)

        @pl.when(t == NORM0 - 1)
        def _():
            tables()

        @pl.when(t == READY)
        def _():
            own_rows[1].wait()
            own_rows[2].wait()
            wait_for(xn.at[0], xsem.at[1])

        @pl.when((t == READY) | (t == READY + 2))
        def _():
            qk_step((t - READY) // 2)

        @pl.when((t == READY + 1) | (t == READY + 3))
        def _():
            v_step((t - READY - 1) // 2)

        @pl.when((t == READY + 1) | (t == READY + 4))
        def _():
            retain((t - READY - 1) // 3)

        @pl.when(t == READY + 5)
        def _():
            out_partner()

        @pl.when(t == READY + 6)
        def _():
            out_own()

        @pl.when(t == READY + 7)
        def _():
            middle()

        @pl.when((t >= GU0) & (t < GU0 + FFC) & ((t - GU0) % 2 == 0))
        def _():
            gu_step(t - GU0, pre_a, pre_b)

        @pl.when((t >= GU0) & (t < GU0 + FFC) & ((t - GU0) % 2 == 1))
        def _():
            gu_step(t - GU0, pre_b, pre_a)

        @pl.when(t == GU0 + FFC)
        def _():
            lax.fori_loop(0, 2, lambda half, _: (gu_conv(FFC - 1, half, pre_a), 0)[1], 0)

        @pl.when(t == LAST - 3)
        def _():
            down_part(0, 3)

        @pl.when(t == LAST - 1)
        def _():
            down_part(3, 2)

        @pl.when(t == LAST)
        def _():
            down_last()

        return 0

    lax.fori_loop(0, LAST + 1, step, 0)
    wait_for(out, osem)
    drain()


def deliver(a, b, held, sems):
    pieces = [pl.ds(i * 128, 128) for i in range(4)]
    for i, r in enumerate(pieces):
        pltpu.make_async_copy(a.at[r], held.at[r], sems.at[i]).start()
    for i, r in enumerate(pieces):
        pltpu.make_async_copy(a.at[r], held.at[r], sems.at[i]).wait()
        pltpu.make_async_copy(held.at[r], b.at[r], sems.at[4 + i]).start()
    for i, r in enumerate(pieces):
        pltpu.make_async_copy(held.at[r], b.at[r], sems.at[4 + i]).wait()


def angle_tables():
    inverse = 10000.0 ** (-np.arange(64) * 2.0 / 128)
    angles = np.arange(LENGTH)[:, None] * inverse[None, :]
    cos, sin = np.cos(angles), np.sin(angles)
    return (
        np.concatenate([cos, cos], axis=1).astype(np.float32),
        np.concatenate([-sin, sin], axis=1).astype(np.float32),
    )


def body(
    tokens, mix_gain, w_query, w_key, w_value, w_out, ffn_gain, w_ffgate, w_ffup, conv_gate, conv_up, w_down
):
    cos, sin = angle_tables()
    vmem = pl.BlockSpec(memory_space=pltpu.VMEM)
    hbm = pl.BlockSpec(memory_space=pl.ANY)
    whole = jax.ShapeDtypeStruct((HALF, D), BF16)
    done = pl.pallas_call(
        layer,
        out_shape=whole,
        in_specs=[hbm] * 10 + [vmem] * 4,
        out_specs=hbm,
        scratch_shapes=[
            pltpu.VMEM((C, 2, 4, 4, 64, COLS), BF16),
            pltpu.VMEM((HALF, D), BF16),
            pltpu.VMEM((HALF, D), BF16),
            pltpu.VMEM((LENGTH, 128), F32),
            pltpu.VMEM((LENGTH, 128), F32),
            pltpu.VMEM((2, HALF, D), BF16),
            pltpu.VMEM((LENGTH, 128), BF16),
            pltpu.VMEM((LENGTH, 128), BF16),
            pltpu.VMEM((LENGTH, 256), BF16),
            pltpu.VMEM((2, 4, 128, 128), F32),
            pltpu.VMEM((2, LENGTH, 256), BF16),
            pltpu.VMEM((HALF, D), BF16),
            pltpu.VMEM((HALF, D), BF16),
            pltpu.VMEM((8 + LENGTH, 256), F32),
            pltpu.VMEM((8 + LENGTH, 256), F32),
            pltpu.VMEM((6, 2, HALF, 256), BF16),
            pltpu.VMEM((2, HALF, D), F32),
            pltpu.SemaphoreType.DMA((10,)),
            pltpu.SemaphoreType.DMA((C, 3)),
            pltpu.SemaphoreType.DMA((len(GROUPS), 4)),
            pltpu.SemaphoreType.DMA((8,)),
            pltpu.SemaphoreType.DMA((8,)),
            pltpu.SemaphoreType.DMA((8,)),
            pltpu.SemaphoreType.DMA,
        ],
        compiler_params=pltpu.CompilerParams(
            collective_id=0, has_side_effects=True, vmem_limit_bytes=VLIM
        ),
    )(
        w_query, w_key, w_value, w_out.T, w_ffgate, w_ffup, w_down.T,
        tokens, jnp.asarray(cos), jnp.asarray(sin), mix_gain.reshape(1, D), ffn_gain.reshape(1, D), conv_gate, conv_up,
    )
    return pl.pallas_call(
        deliver,
        out_shape=whole,
        in_specs=[hbm],
        out_specs=hbm,
        scratch_shapes=[pltpu.VMEM((HALF, D), BF16), pltpu.SemaphoreType.DMA((8,))],
        compiler_params=pltpu.CompilerParams(vmem_limit_bytes=67043328),
    )(done)


def solution(mesh):
    w = P("fs", "tp")
    placed = (P(("rep", "fs", "tp"), None), P(), w, w, w, P("tp", "fs"), P(), w, w, P(), P(), P("tp", "fs"))
    return jax.shard_map(
        body, mesh=mesh, in_specs=placed, out_specs=P(("rep", "fs", "tp"), None), check_vma=False
    )
```
